128 devices in a mesh: sp: 32 (over z, y, core), tp: 4 (over x).
Axes of the slice: x: 4, y: 4, z: 4, core: 2. Of those that a mesh axis runs over, the one named last changes fastest.
Arguments:
- tokens: bfloat16 [16384, 2048], P(('sp', 'tp')), may hold values from -6 to 6
- norm_gain: float32 [2048], replicated, may hold values from 0.1 to 1.9
- query_weight: bfloat16 [2048, 1024], P(None, 'tp'), may hold values from -0.13258252 to 0.13258252
- key_weight: bfloat16 [2048, 1024], P(None, 'tp'), may hold values from -0.13258252 to 0.13258252
- value_weight: bfloat16 [2048, 1024], P(None, 'tp'), may hold values from -0.125 to 0.125
- glu_value_weight: bfloat16 [2048, 1024], P(None, 'tp'), may hold values from -0.125 to 0.125
- glu_gate_weight: bfloat16 [2048, 1024], P(None, 'tp'), may hold values from -0.125 to 0.125
- qk_gain: float32 [2, 64], replicated, may hold values from 1 to 6
- mix_lambda: float32 [8], P('tp'), may hold values from 0.3 to 0.8
- head_gain: float32 [128], replicated, may hold values from 0.1 to 1.9
- conv_kernel: float32 [31, 1024], P(None, 'tp'), may hold values from -1 to 1
- channel_gain: float32 [1024], P('tp'), may hold values from 0.1 to 1.9
- channel_shift: float32 [1024], P('tp'), may hold values from -3 to 3
- output_weight: bfloat16 [2048, 2048], replicated, may hold values from -0.125 to 0.125
Outputs:
- mixed: bfloat16 [16384, 2048], P(('sp', 'tp'))
- log_totals: float32 [2, 8, 16384], P(None, 'tp', 'sp')
The draws below stay inside these ranges and needn't reach their ends.
All inputs are finite; a program needn't handle non-finite values.
Results may differ from the reference program's by a relative error of at most 0.035.
Values may be sent and summed in bfloat16 or wider, within the bound.
A program may use at most 128 MiB of HBM per device.

```python
import jax
import jax.numpy as jnp
from jax import lax

D = 2048
HEADS = 8
HEAD_DIM = 64
VDIM = 128
CONV = 1024
KERNEL = 31
TOKENS = 16384
MIX = 2048


def draw_qk_gain(key, part):
    spread = jax.random.uniform(jax.random.fold_in(key, 7), (2, HEAD_DIM), jnp.float32, -1.0, 1.0)
    return 1.3 + 0.25 * spread


def paired_weights(key):
    columns = HEADS * 2 * HEAD_DIM
    factor = D ** (-0.5)
    limit = 6.0 * factor
    shared = jax.random.normal(jax.random.fold_in(key, 11), (D, columns), jnp.float32) * factor
    separate = jax.random.normal(jax.random.fold_in(key, 12), (D, columns), jnp.float32) * factor
    shared = jnp.clip(shared, -limit, limit)
    separate = jnp.clip(separate, -limit, limit)
    return (shared, separate)


def draw_query_weight(key, part):
    shared, separate = paired_weights(key)
    return shared.astype(jnp.bfloat16)


def draw_key_weight(key, part):
    shared, separate = paired_weights(key)
    return separate.astype(jnp.bfloat16)


def block_levels(rng, dims, pieces, low, largest):
    def one(position, blocks):
        draws = jax.random.uniform(jax.random.fold_in(jax.random.fold_in(rng, 6), position), (blocks,), jnp.float32, low / len(pieces), largest / len(pieces))
        return jnp.repeat(jnp.exp(draws), dims[position] // blocks).reshape((-1,) + (1,) * (len(dims) - position - 1))

    factor_of = one(*pieces[0])
    for cut in pieces[1:]:
        factor_of = factor_of * one(*cut)
    return factor_of


def normal_values(own_key, shape, width, most, split=(), held_as=jnp.bfloat16):
    drawn = width * jax.random.normal(own_key, shape, jnp.float32)
    if split:
        drawn = drawn * block_levels(own_key, shape, split, -0.22, 0.18)
    return jnp.clip(drawn, -most, most).astype(held_as)


def setup_inputs(seed: int = 0) -> dict:
    splits = jax.random.split(jax.random.key(seed), 15)
    tokens = normal_values(splits[0], (TOKENS, D), 1.0, 6.0, ((0, 128),))
    norm_gain = jnp.clip(1.0 + 0.18 * jax.random.normal(splits[1], (D,), jnp.float32), 0.1, 1.9)
    query_weight = draw_query_weight(jax.random.fold_in(splits[14], 71), 0)
    key_weight = draw_key_weight(jax.random.fold_in(splits[14], 71), 0)
    value_weight = normal_values(splits[4], (D, HEADS * VDIM), D ** -0.5, 0.125, ((1, 4),))
    glu_value_weight = normal_values(splits[5], (D, CONV), D ** -0.5, 0.125, ((1, 4),))
    glu_gate_weight = normal_values(splits[6], (D, CONV), D ** -0.5, 0.125, ((1, 4),))
    qk_gain = draw_qk_gain(jax.random.fold_in(splits[14], 71), 0)
    mix_lambda = jnp.clip(0.3 + 0.5 * jax.random.uniform(splits[8], (HEADS,), jnp.float32) ** block_levels(splits[8], (HEADS,), ((0, 4),), -0.2, 0.2), 0.3, 0.8)
    head_gain = jnp.clip(1.0 + 0.18 * jax.random.normal(splits[9], (VDIM,), jnp.float32), 0.1, 1.9)
    conv_kernel = normal_values(splits[10], (KERNEL, CONV), KERNEL ** -0.5, 1.0, ((1, 4),), jnp.float32)
    channel_gain = jnp.clip(1.0 + 0.18 * jax.random.normal(splits[11], (CONV,), jnp.float32), 0.1, 1.9)
    channel_shift = normal_values(splits[12], (CONV,), 0.5, 3.0, ((0, 4),), jnp.float32)
    output_weight = normal_values(splits[13], (MIX, D), MIX ** -0.5, 0.125)
    return dict(tokens=tokens, norm_gain=norm_gain, query_weight=query_weight, key_weight=key_weight, value_weight=value_weight, glu_value_weight=glu_value_weight, glu_gate_weight=glu_gate_weight, qk_gain=qk_gain, mix_lambda=mix_lambda, head_gain=head_gain, conv_kernel=conv_kernel, channel_gain=channel_gain, channel_shift=channel_shift, output_weight=output_weight)


def rotate(values, positions):
    half = values.shape[-1] // 2
    inverse = 10000.0 ** (-jnp.arange(0, half, dtype=jnp.float32) * 2.0 / values.shape[-1])
    angles = positions[:, None] * inverse[None, :]
    cosine = jnp.cos(angles)[:, None, None, :]
    sine = jnp.sin(angles)[:, None, None, :]
    first = values[..., :half]
    second = values[..., half:]
    return jnp.concatenate([first * cosine - second * sine, second * cosine + first * sine], axis=-1)

def prepare(raw, qk_gain, positions):
    values = raw.astype(jnp.float32)
    values = values * lax.rsqrt(lax.optimization_barrier(jnp.mean(values * values, axis=-1, keepdims=True)) + 1e-06)
    values = values * qk_gain[None, None, :, :]
    return rotate(values, positions).astype(jnp.bfloat16)

def reference(tokens, norm_gain, query_weight, key_weight, value_weight, glu_value_weight, glu_gate_weight, qk_gain, mix_lambda, head_gain, conv_kernel, channel_gain, channel_shift, output_weight):
    inputs = tokens.astype(jnp.float32)
    normed = (inputs * lax.rsqrt(lax.optimization_barrier(jnp.mean(inputs * inputs, axis=-1, keepdims=True)) + 1e-06) * norm_gain).astype(jnp.bfloat16)
    queries = jnp.dot(normed, query_weight, preferred_element_type=jnp.float32).astype(jnp.bfloat16).reshape(TOKENS, HEADS, 2, HEAD_DIM)
    keys = jnp.dot(normed, key_weight, preferred_element_type=jnp.float32).astype(jnp.bfloat16).reshape(TOKENS, HEADS, 2, HEAD_DIM)
    values = jnp.dot(normed, value_weight, preferred_element_type=jnp.float32).astype(jnp.bfloat16).reshape(TOKENS, HEADS, VDIM)
    glu_a = jnp.dot(normed, glu_value_weight, preferred_element_type=jnp.float32).astype(jnp.bfloat16)
    glu_g = jnp.dot(normed, glu_gate_weight, preferred_element_type=jnp.float32).astype(jnp.bfloat16)
    positions = jnp.arange(TOKENS, dtype=jnp.int32)
    rq = prepare(queries, qk_gain, positions.astype(jnp.float32))
    rk = prepare(keys, qk_gain, positions.astype(jnp.float32))
    key_heads = jnp.transpose(rk, (1, 0, 2, 3)).astype(jnp.float32)
    value_heads = jnp.transpose(values, (1, 0, 2)).astype(jnp.float32)
    block = 512
    blocks = TOKENS // block
    query_blocks = rq.reshape(blocks, block, HEADS, 2, HEAD_DIM)
    starts = jnp.arange(blocks, dtype=jnp.int32) * block
    scale = HEAD_DIM ** (-0.5)

    def one_block(item):
        query_block, begin = item
        query_pos = begin + jnp.arange(block, dtype=jnp.int32)
        allowed = positions[None, :] <= query_pos[:, None]

        def one_head(head_item):
            query_head, key_head, value_head, weight_two = head_item
            scores = jnp.einsum('qmd,kmd->mqk', query_head.astype(jnp.float32), key_head) * scale
            scores = jnp.where(allowed[None], scores, -1e+30)
            top = lax.optimization_barrier(jnp.max(scores, axis=-1))
            probs = jnp.where(allowed[None], jnp.exp(scores - top[..., None]), 0.0)
            total = lax.optimization_barrier(jnp.sum(probs, axis=-1))
            rounded = probs.astype(jnp.bfloat16).astype(jnp.float32)
            summed = jnp.einsum('mqk,kd->mqd', rounded, value_head)
            heads_out = summed[0] / total[0][:, None] - weight_two * summed[1] / total[1][:, None]
            heads_out = heads_out * lax.rsqrt(lax.optimization_barrier(jnp.mean(heads_out * heads_out, axis=-1, keepdims=True)) + 1e-06) * head_gain
            return (heads_out.astype(jnp.bfloat16), top + jnp.log(total))
        return lax.map(one_head, (jnp.transpose(query_block, (1, 0, 2, 3)), key_heads, value_heads, mix_lambda))
    outputs, totals = lax.map(one_block, (query_blocks, starts))
    attended = jnp.transpose(outputs, (0, 2, 1, 3)).reshape(TOKENS, HEADS * VDIM)
    log_totals = jnp.transpose(totals, (2, 1, 0, 3)).reshape(2, HEADS, TOKENS)
    gated = (glu_a.astype(jnp.float32) * jax.nn.sigmoid(glu_g.astype(jnp.float32))).astype(jnp.bfloat16)
    padded = jnp.concatenate([jnp.zeros((KERNEL - 1, CONV), jnp.float32), gated.astype(jnp.float32)], axis=0)
    convolved = jnp.zeros((TOKENS, CONV), jnp.float32)
    for offset in range(KERNEL):
        convolved = convolved + conv_kernel[offset][None, :] * padded[offset:offset + TOKENS]
    middle = lax.optimization_barrier(jnp.mean(convolved, axis=-1, keepdims=True))
    spread = lax.optimization_barrier(jnp.mean(convolved * convolved, axis=-1, keepdims=True)) - middle * middle
    conv_out = jax.nn.silu((convolved - middle) * lax.rsqrt(spread + 1e-05) * channel_gain + channel_shift).astype(jnp.bfloat16)
    merged = jnp.concatenate([attended, conv_out], axis=1)
    mixed = jnp.dot(merged, output_weight, preferred_element_type=jnp.float32).astype(jnp.bfloat16)
    return (mixed, log_totals)
```

```python
import jax
import jax.numpy as jnp
from jax import lax
from jax.experimental import pallas as pl
from jax.experimental.pallas import tpu as pltpu
from jax.sharding import PartitionSpec as P


MESH = pl.DeviceIdType.MESH
LOG2E = 1.4426950408889634
NEG = -1e30


def place(half, chip_z, chip_y):
    total = lax.rem(chip_y + chip_z, 4)
    row = chip_y + half * (chip_z - chip_y)
    return row * 4 + total


def chip_at(half, position):
    row = position // 4
    other = lax.rem(lax.rem(position, 4) + 4 - row, 4)
    chip_y = row + half * (other - row)
    chip_z = other + half * (row - other)
    return chip_z * 4 + chip_y


def attend_kernel(
    own_ref, even_ref, odd_ref, lam_ref, gain_ref,
    att_ref, lse_ref,
    kv, odd_in, queries, tops, totals, summed,
    load_sem, odd_send, odd_recv, ring_send, ring_recv, twin_send, twin_recv,
):
    me = lax.axis_index("sp")
    core = lax.rem(me, 2)
    chip = me // 2
    chip_z, chip_y = chip // 4, lax.rem(chip, 4)
    twin = me + 1 - 2 * core
    partner = 31 - me

    def origin(half, direction, step):
        here = place(half, chip_z, chip_y)
        there = lax.rem(here + 16 - step + 2 * step * direction, 16)
        return chip_at(half, there)

    def onward(half, direction):
        here = place(half, chip_z, chip_y)
        there = lax.rem(here + 17 - 2 * direction, 16)
        return chip_at(half, there) * 2 + core

    def ring_copy(ring, step, sub):
        half, direction = ring // 2, ring % 2
        source = origin(half, direction, step - 1) * 2 + core
        piece = kv.at[2 * source + half, sub]
        return pltpu.make_async_remote_copy(
            src_ref=piece, dst_ref=piece,
            send_sem=ring_send.at[ring, step - 1, sub],
            recv_sem=ring_recv.at[ring, step - 1, sub],
            device_id={"sp": onward(half, direction)}, device_id_type=MESH,
        )

    def ring_arrival(ring, step, sub):
        half, direction = ring // 2, ring % 2
        source = origin(half, direction, step) * 2 + core
        piece = kv.at[2 * source + half, sub]
        return pltpu.make_async_remote_copy(
            src_ref=piece, dst_ref=piece,
            send_sem=ring_send.at[ring, step - 1, sub],
            recv_sem=ring_recv.at[ring, step - 1, sub],
            device_id={"sp": onward(half, direction)}, device_id_type=MESH,
        )

    def twin_copy(ring, step, sender):
        half, direction = ring // 2, ring % 2
        source = origin(half, direction, step) * 2 + sender
        piece = kv.at[2 * source + half]
        return pltpu.make_async_remote_copy(
            src_ref=piece, dst_ref=piece,
            send_sem=twin_send.at[ring, step],
            recv_sem=twin_recv.at[ring, step],
            device_id={"sp": twin}, device_id_type=MESH,
        )

    loads = []
    for half in range(2):
        loads.append(
            pltpu.make_async_copy(own_ref.at[half], kv.at[2 * me + half], load_sem.at[half])
        )
        loads[-1].start()

    barrier = pltpu.get_barrier_semaphore()
    for ring in range(4):
        pl.semaphore_signal(
            barrier, inc=1, device_id={"sp": onward(ring // 2, ring % 2)}, device_id_type=MESH
        )
    pl.semaphore_signal(barrier, inc=1, device_id={"sp": twin}, device_id_type=MESH)
    pl.semaphore_signal(barrier, inc=1, device_id={"sp": partner}, device_id_type=MESH)

    for chunk in range(2):
        for head in range(2):
            tops[2 * chunk + head] = jnp.full((1, 512), NEG, jnp.float32)
            totals[2 * chunk + head] = jnp.zeros((1, 512), jnp.float32)
            summed[2 * chunk + head] = jnp.zeros((128, 512), jnp.float32)

    def spread(chunk, head, block):
        rows = lax.broadcasted_iota(jnp.int32, (128, 256), 0)
        zero = jnp.zeros((128, 256), jnp.bfloat16)
        queries[2 * chunk + head, :, 0:256] = jnp.where(rows < 64, block, zero)
        queries[2 * chunk + head, :, 256:512] = jnp.where(rows < 64, zero, block)

    for copy in loads:
        copy.wait()
    pl.semaphore_wait(barrier, 6)

    for sub in range(4):
        for ring in range(4):
            ring_copy(ring, 1, sub).start()
    odd_copy = pltpu.make_async_remote_copy(
        src_ref=odd_ref, dst_ref=odd_in, send_sem=odd_send, recv_sem=odd_recv,
        device_id={"sp": partner}, device_id_type=MESH,
    )
    odd_copy.start()
    for half in range(2):
        twin_copy(2 * half, 0, core).start()

    for head in range(2):
        spread(0, head, even_ref[head])
    odd_copy.wait_recv()
    for head in range(2):
        spread(1, head, odd_in[head])

    def advance(chunk, block, masked):
        for head in range(2):
            lanes = slice(128 * head, 128 * head + 128)
            state = 2 * chunk + head
            keys = jnp.concatenate([kv[block, 0, :, lanes], kv[block, 1, :, lanes]], axis=0)
            scores = jnp.dot(keys, queries[state], preferred_element_type=jnp.float32)
            if masked:
                key_pos = lax.broadcasted_iota(jnp.int32, (256, 512), 0)
                query_pos = lax.broadcasted_iota(jnp.int32, (256, 512), 1) & 255
                scores = jnp.where(key_pos <= query_pos, scores, NEG)
            before = tops[state]
            top = jnp.maximum(before, jnp.max(scores, axis=0, keepdims=True))
            weights = jnp.exp2(scores - top)
            factor = jnp.exp2(before - top)
            totals[state] = totals[state] * factor + jnp.sum(weights, axis=0, keepdims=True)
            added = jnp.dot(
                kv[block, 2 + head], weights.astype(jnp.bfloat16),
                preferred_element_type=jnp.float32,
            )
            summed[state] = summed[state] * factor + added
            tops[state] = top

    def consider(chunk, block):
        last = 2 * me + chunk * (63 - 4 * me)

        @pl.when(block < last)
        def _():
            advance(chunk, block, False)

        @pl.when(block == last)
        def _():
            advance(chunk, block, True)

    def work(ring, step):
        half, direction = ring // 2, ring % 2
        source = origin(half, direction, step) * 2

        def item(j, _):
            turn, chunk = j // 2, lax.rem(j, 2)
            sender = core + turn * (1 - 2 * core)

            @pl.when(j == 2)
            def _():
                twin_copy(ring, step, 1 - core).wait_recv()

            consider(chunk, 2 * (source + sender) + half)
            return 0

        lax.fori_loop(0, 4, item, 0)

    def turn(t, _):
        step, sub = t // 4 + 1, lax.rem(t, 4)
        for ring in range(4):
            ring_arrival(ring, step, sub).wait_recv()

            @pl.when((step < 7) | (sub // 2 == ring % 2))
            def _():
                ring_copy(ring, step + 1, sub).start()

        @pl.when(sub == 3)
        def _():
            for ring in range(4):
                twin_copy(ring, step, core).start()

        @pl.when((step > 1) | (lax.rem(sub, 2) == 0))
        def _():
            work(sub, step - 1)

        return 0

    lax.fori_loop(0, 28, turn, 0)

    for half in range(2):
        for sub in range(4):
            ring_arrival(2 * half + sub // 2, 8, sub).wait_recv()
        twin_copy(2 * half, 8, core).start()
    lax.fori_loop(0, 4, lambda r, _: (work(r, 7), 0)[1], 0)
    lax.fori_loop(0, 2, lambda h, _: (work(2 * h, 8), 0)[1], 0)

    for chunk in range(2):
        for head in range(2):
            state = 2 * chunk + head
            share = summed[state] / totals[state]
            out = share[:, 0:256] - lam_ref[head] * share[:, 256:512]
            power = jnp.mean(out * out, axis=0, keepdims=True)
            out = out * lax.rsqrt(power + 1e-06) * gain_ref[...]
            att_ref[chunk, :, 128 * head : 128 * head + 128] = out.T.astype(jnp.bfloat16)
            lse_ref[chunk, head] = (tops[state] + jnp.log2(totals[state])) * (1.0 / LOG2E)

    odd_copy.wait_send()
    for half in range(2):
        twin_copy(2 * half, 0, core).wait_send()
        twin_copy(2 * half, 8, core).wait_send()

    def drain(step, _):
        for ring in range(4):
            twin_copy(ring, step, core).wait_send()
            for sub in range(4):
                ring_copy(ring, step, sub).wait_send()
        return 0

    lax.fori_loop(1, 8, drain, 0)
    for half in range(2):
        for sub in range(4):
            ring_copy(2 * half + sub // 2, 8, sub).wait_send()


def attend(own, even, odd, lam, gain):
    vmem = pl.BlockSpec(memory_space=pltpu.VMEM)
    return pl.pallas_call(
        attend_kernel,
        out_shape=(
            jax.ShapeDtypeStruct((2, 256, 256), jnp.bfloat16),
            jax.ShapeDtypeStruct((2, 2, 1, 512), jnp.float32),
        ),
        in_specs=[pl.BlockSpec(memory_space=pl.ANY), vmem, vmem, vmem, vmem],
        out_specs=(vmem, vmem),
        scratch_shapes=[
            pltpu.VMEM((64, 4, 128, 256), jnp.bfloat16),
            pltpu.VMEM((2, 128, 256), jnp.bfloat16),
            pltpu.VMEM((4, 128, 512), jnp.bfloat16),
            pltpu.VMEM((4, 1, 512), jnp.float32),
            pltpu.VMEM((4, 1, 512), jnp.float32),
            pltpu.VMEM((4, 128, 512), jnp.float32),
            pltpu.SemaphoreType.DMA((2,)),
            pltpu.SemaphoreType.DMA,
            pltpu.SemaphoreType.DMA,
            pltpu.SemaphoreType.DMA((4, 8, 4)),
            pltpu.SemaphoreType.DMA((4, 8, 4)),
            pltpu.SemaphoreType.DMA((4, 9)),
            pltpu.SemaphoreType.DMA((4, 9)),
        ],
        compiler_params=pltpu.CompilerParams(
            collective_id=0, has_side_effects=True, vmem_limit_bytes=40 * 1024 * 1024
        ),
    )(own, even, odd, lam, gain)


def joined_along(tiles, dim):
    dims = list(tiles.shape[1:])
    dims[dim] *= tiles.shape[0]
    return jnp.moveaxis(tiles, 0, dim).reshape(dims)


def sent_to_all(shard, axis):
    copies = jnp.broadcast_to(shard, (lax.axis_size(axis), *shard.shape))
    return lax.all_to_all(copies, axis, split_axis=0, concat_axis=0, tiled=True)


def collect(shard, axis, dim):
    return joined_along(sent_to_all(shard, axis), dim)


def from_behind(value, axis, steps):
    count = lax.axis_size(axis)
    leading, last = (max(0, -steps), min(count, count - steps))
    return lax.ppermute(value, axis, [(source, source + steps) for source in range(leading, last)])


def over_copies(shard, axis):
    everything = sent_to_all(shard, axis)
    return jnp.sum(everything, axis=0)


def in_one(arrays, axis):
    ends = [0]
    for a in arrays:
        ends.append(ends[-1] + a.size)
    total = over_copies(jnp.concatenate([a.ravel() for a in arrays]), axis)
    return tuple((total[b:e].reshape(a.shape) for a, b, e in zip(arrays, ends, ends[1:])))


def rotate(values, positions):
    half = values.shape[-1] // 2
    inverse = 10000.0 ** (-jnp.arange(0, half, dtype=jnp.float32) * 2.0 / values.shape[-1])
    angles = positions[:, None] * inverse[None, :]
    cosine = jnp.cos(angles)[:, None, None, :]
    sine = jnp.sin(angles)[:, None, None, :]
    first = values[..., :half]
    second = values[..., half:]
    return jnp.concatenate(
        [first * cosine - second * sine, second * cosine + first * sine], axis=-1
    )


def prepare(raw, qk_gain, positions, factor=1.0):
    values = raw.astype(jnp.float32)
    values = values * lax.rsqrt(jnp.mean(values * values, axis=-1, keepdims=True) + 1e-06)
    values = values * qk_gain[None, None, :, :]
    return (rotate(values, positions) * factor).astype(jnp.bfloat16)


def per_device(
    tokens,
    norm_gain,
    query_weight,
    key_weight,
    value_weight,
    glu_value_weight,
    glu_gate_weight,
    qk_gain,
    mix_lambda,
    head_gain,
    conv_kernel,
    channel_gain,
    channel_shift,
    output_weight,
):
    head_size = qk_gain.shape[1]
    heads_here = mix_lambda.shape[0]
    value_size = head_gain.shape[0]
    kernel_len = conv_kernel.shape[0]
    conv_here = conv_kernel.shape[1]
    width = tokens.shape[1]
    matrices = (query_weight, key_weight, value_weight, glu_value_weight, glu_gate_weight)

    def project(piece):
        inputs = piece.astype(jnp.float32)
        normed = (
            inputs
            * lax.rsqrt(jnp.mean(inputs * inputs, axis=-1, keepdims=True) + 1e-06)
            * norm_gain
        ).astype(jnp.bfloat16)
        results = [
            jnp.dot(normed, matrix, preferred_element_type=jnp.float32).astype(jnp.bfloat16)
            for matrix in matrices
        ]
        return jnp.concatenate(results, axis=1)

    projected = project(collect(tokens, "tp", 0))
    tok_rows = projected.shape[0]
    bounds = [0]
    for matrix in matrices:
        bounds.append(bounds[-1] + matrix.shape[1])
    queries = projected[:, bounds[0] : bounds[1]].reshape(tok_rows, heads_here, 2, head_size)
    keys = projected[:, bounds[1] : bounds[2]].reshape(tok_rows, heads_here, 2, head_size)
    values = projected[:, bounds[2] : bounds[3]].reshape(tok_rows, heads_here, value_size)
    glu_a = projected[:, bounds[3] : bounds[4]]
    glu_g = projected[:, bounds[4] : bounds[5]]
    offset = lax.axis_index("sp") * tok_rows
    query_pos = offset + jnp.arange(tok_rows, dtype=jnp.int32)
    float_pos = query_pos.astype(jnp.float32)
    scale = head_size ** (-0.5) * LOG2E
    rq = prepare(queries, qk_gain, float_pos, scale).reshape(2, 256, heads_here, 2 * head_size)
    rq = jnp.transpose(rq, (0, 2, 3, 1))
    rk = prepare(keys, qk_gain, float_pos).reshape(2, 2, 128, heads_here * 2 * head_size)
    flipped = jnp.transpose(values.reshape(2, 256, heads_here, value_size), (0, 2, 3, 1))
    own = jnp.concatenate([rk, flipped], axis=1)
    att, lse = attend(own, rq[0], rq[1], mix_lambda[:, None, None], head_gain[:, None])
    count = lax.axis_size("sp")
    swap = [(i, count - 1 - i) for i in range(count)]
    attended = jnp.concatenate([att[0], lax.ppermute(att[1], "sp", swap)], axis=0)
    logs = jnp.stack([lse[0], lax.ppermute(lse[1], "sp", swap)], axis=0)
    logs = logs.reshape(2, heads_here, 2, 256)
    log_totals = jnp.transpose(logs, (2, 1, 0, 3)).reshape(2, heads_here, tok_rows)
    gated = (glu_a.astype(jnp.float32) * jax.nn.sigmoid(glu_g.astype(jnp.float32))).astype(
        jnp.bfloat16
    )
    earlier = from_behind(gated[tok_rows - (kernel_len - 1) :], "sp", 1)
    extended = jnp.concatenate([earlier, gated], axis=0).astype(jnp.float32)
    convolved = jnp.zeros((tok_rows, conv_here), jnp.float32)
    for step in range(kernel_len):
        convolved = convolved + conv_kernel[step][None, :] * extended[step : step + tok_rows]
    plain_sum, square_sum = in_one(
        (jnp.sum(convolved, axis=1), jnp.sum(convolved * convolved, axis=1)), "tp"
    )
    channels = conv_here * lax.axis_size("tp")
    middle = (plain_sum / channels)[:, None]
    spread = (square_sum / channels)[:, None] - middle * middle
    conv_out = jax.nn.silu(
        (convolved - middle) * lax.rsqrt(spread + 1e-05) * channel_gain + channel_shift
    ).astype(jnp.bfloat16)
    merged = jnp.concatenate([attended, conv_out], axis=1)
    groups = lax.axis_size("tp")
    branch_width = heads_here * value_size
    weight_view = output_weight.reshape(2, groups, branch_width, width)
    moved = lax.all_to_all(merged, "tp", split_axis=0, concat_axis=1, tiled=True)
    arranged = moved.reshape(tok_rows // groups, groups, 2, branch_width)
    mixed = jnp.einsum(
        "rtcj,ctjd->rd", arranged, weight_view, preferred_element_type=jnp.float32
    ).astype(jnp.bfloat16)
    return (mixed, log_totals)


def solution(mesh):
    placed = (
        P(("sp", "tp"), None),
        P(),
        P(None, "tp"),
        P(None, "tp"),
        P(None, "tp"),
        P(None, "tp"),
        P(None, "tp"),
        P(),
        P("tp"),
        P(),
        P(None, "tp"),
        P("tp"),
        P("tp"),
        P(),
    )
    return jax.shard_map(
        per_device,
        mesh=mesh,
        in_specs=placed,
        out_specs=(P(("sp", "tp"), None), P(None, "tp", "sp")),
        check_vma=False,
    )
```

```python
import jax
import jax.numpy as jnp
from jax import lax
from jax.experimental import pallas as pl
from jax.experimental.pallas import tpu as pltpu
from jax.sharding import PartitionSpec as P

MESH = pl.DeviceIdType.MESH
LOG2E = 1.4426950408889634
NEG = -1e30
SUBS = 4
SUB_ROWS = 512 // SUBS


def place(half, chip_z, chip_y):
    total = lax.rem(chip_y + chip_z, 4)
    row = chip_y + half * (chip_z - chip_y)
    return row * 4 + total


def chip_at(half, position):
    row = position // 4
    other = lax.rem(lax.rem(position, 4) + 4 - row, 4)
    chip_y = row + half * (other - row)
    chip_z = other + half * (row - other)
    return chip_z * 4 + chip_y


def attend_kernel(
    own_ref, query_ref, gated_ref, lam_ref, gain_ref, taps_ref, scale_ref, shift_ref, out_w_ref,
    mixed_ref, logs_ref,
    kv, odd_in, queries, tops, totals, summed,
    halo, shifted, convolved, sums, conv_out, conv_in, attended, attended_in, logs_in, out_w, mixing,
    load_sem, odd_send, odd_recv, ring_send, ring_recv, twin_send, twin_recv,
    weight_sem, halo_sem, sums_send, sums_recv, conv_send, conv_recv, att_send, att_recv, logs_sem,
):
    me = lax.axis_index("sp")
    group = lax.axis_index("tp")
    core = lax.rem(me, 2)
    chip = me // 2
    chip_z, chip_y = chip // 4, lax.rem(chip, 4)
    twin = me + 1 - 2 * core
    partner = 31 - me

    def origin(half, direction, step):
        here = place(half, chip_z, chip_y)
        there = lax.rem(here + 16 - step + 2 * step * direction, 16)
        return chip_at(half, there)

    def onward(half, direction):
        here = place(half, chip_z, chip_y)
        there = lax.rem(here + 17 - 2 * direction, 16)
        return chip_at(half, there) * 2 + core

    def ring_copy(ring, step, sub):
        half, direction = ring // 2, ring % 2
        source = origin(half, direction, step - 1) * 2 + core
        piece = kv.at[2 * source + half, pl.ds(sub * SUB_ROWS, SUB_ROWS)]
        return pltpu.make_async_remote_copy(
            src_ref=piece, dst_ref=piece,
            send_sem=ring_send.at[ring, step - 1, sub],
            recv_sem=ring_recv.at[ring, step - 1, sub],
            device_id={"sp": onward(half, direction)}, device_id_type=MESH,
        )

    def ring_arrival(ring, step, sub):
        half, direction = ring // 2, ring % 2
        source = origin(half, direction, step) * 2 + core
        piece = kv.at[2 * source + half, pl.ds(sub * SUB_ROWS, SUB_ROWS)]
        return pltpu.make_async_remote_copy(
            src_ref=piece, dst_ref=piece,
            send_sem=ring_send.at[ring, step - 1, sub],
            recv_sem=ring_recv.at[ring, step - 1, sub],
            device_id={"sp": onward(half, direction)}, device_id_type=MESH,
        )

    def twin_copy(ring, step, sender):
        half, direction = ring // 2, ring % 2
        source = origin(half, direction, step) * 2 + sender
        piece = kv.at[2 * source + half]
        return pltpu.make_async_remote_copy(
            src_ref=piece, dst_ref=piece,
            send_sem=twin_send.at[ring, step],
            recv_sem=twin_recv.at[ring, step],
            device_id={"sp": twin}, device_id_type=MESH,
        )

    loads = []
    for half in range(2):
        loads.append(
            pltpu.make_async_copy(own_ref.at[half], kv.at[2 * me + half], load_sem.at[half])
        )
        loads[-1].start()

    fetch = pltpu.make_async_copy(out_w_ref, out_w, weight_sem)
    fetch.start()

    barrier = pltpu.get_barrier_semaphore()
    for ring in range(4):
        pl.semaphore_signal(
            barrier, inc=1, device_id={"sp": onward(ring // 2, ring % 2)}, device_id_type=MESH
        )
    pl.semaphore_signal(barrier, inc=1, device_id={"sp": twin}, device_id_type=MESH)
    after, before_me = lax.rem(me + 1, 32), lax.rem(me + 31, 32)
    for place_on_line in (after, before_me):
        pl.semaphore_signal(barrier, inc=1, device_id={"sp": place_on_line}, device_id_type=MESH)
    for hop in range(4):
        peer = lax.rem(group + hop, 4)
        pl.semaphore_signal(
            barrier, inc=1, device_id={"sp": partner, "tp": peer}, device_id_type=MESH
        )
        if hop > 0:
            pl.semaphore_signal(barrier, inc=1, device_id={"tp": peer}, device_id_type=MESH)

    for chunk in range(2):
        for head in range(2):
            tops[2 * chunk + head] = jnp.full((1, 512), NEG, jnp.float32)
            totals[2 * chunk + head] = jnp.zeros((1, 512), jnp.float32)
            summed[2 * chunk + head] = jnp.zeros((128, 512), jnp.float32)

    def spread(chunk, head, block):
        rows = lax.broadcasted_iota(jnp.int32, (128, 256), 0)
        zero = jnp.zeros((128, 256), jnp.bfloat16)
        queries[2 * chunk + head, :, 0:256] = jnp.where(rows < 64, block, zero)
        queries[2 * chunk + head, :, 256:512] = jnp.where(rows < 64, zero, block)

    for copy in loads:
        copy.wait()
    pl.semaphore_wait(barrier, 14)

    for sub in range(SUBS):
        for ring in range(4):
            ring_copy(ring, 1, sub).start()
    odd_copy = pltpu.make_async_remote_copy(
        src_ref=query_ref.at[1], dst_ref=odd_in, send_sem=odd_send, recv_sem=odd_recv,
        device_id={"sp": partner}, device_id_type=MESH,
    )
    odd_copy.start()
    halo_copy = pltpu.make_async_remote_copy(
        src_ref=gated_ref.at[pl.ds(480, 32)], dst_ref=halo,
        send_sem=halo_sem.at[0], recv_sem=halo_sem.at[1],
        device_id={"sp": after}, device_id_type=MESH,
    )
    halo_copy.start()
    for half in range(2):
        twin_copy(2 * half, 0, core).start()

    for head in range(2):
        spread(0, head, query_ref[0, head])
    odd_copy.wait_recv()
    for head in range(2):
        spread(1, head, odd_in[head])

    def to_peers(source, target, send, recv, hop, rows=None):
        peer = lax.rem(group + hop, 4)
        piece = source if rows is None else source.at[pl.ds(pl.multiple_of(rows * peer, 16), rows)]
        return pltpu.make_async_remote_copy(
            src_ref=piece, dst_ref=target.at[4 - hop],
            send_sem=send.at[4 - hop], recv_sem=recv.at[4 - hop],
            device_id={"tp": peer}, device_id_type=MESH,
        )

    def sums_copy(hop):
        return to_peers(sums.at[0], sums, sums_send, sums_recv, hop)

    def conv_copy(hop):
        return to_peers(conv_out, conv_in, conv_send, conv_recv, hop, 128)

    halo_copy.wait_recv()
    first = jnp.where(me == 0, jnp.zeros((32, 256), jnp.float32), halo[...].astype(jnp.float32))
    shifted[0, 0:32, :] = first
    shifted[0, 32:544, :] = gated_ref[...].astype(jnp.float32)
    for shift in range(1, 8):
        shifted[shift, 0:536, :] = shifted[0, shift : shift + 536, :]

    def conv_tile(tile, _):
        base = tile * 32
        total = jnp.zeros((32, 256), jnp.float32)
        for tap in range(31):
            offset = tap + 2
            start = pl.multiple_of(base + offset // 8 * 8, 8)
            total = total + taps_ref[tap : tap + 1, :] * shifted[offset % 8, pl.ds(start, 32), :]
        convolved[pl.ds(pl.multiple_of(base, 32), 32), :] = total
        return 0

    lax.fori_loop(0, 16, conv_tile, 0)
    lanes = lax.broadcasted_iota(jnp.int32, (512, 128), 1)
    conv_now = convolved[...]
    plain = jnp.sum(conv_now, axis=1, keepdims=True)
    square = jnp.sum(conv_now * conv_now, axis=1, keepdims=True)
    both = jnp.where(lanes == 0, plain, jnp.where(lanes == 1, square, 0.0))
    sums[0] = both.T[0:8]

    def normalize():
        for hop in range(1, 4):
            sums_copy(hop).wait_recv()
        total = sums[0] + sums[1] + sums[2] + sums[3]
        padded = jnp.concatenate([total, jnp.zeros((120, 512), jnp.float32)], axis=0).T
        middle = padded[:, 0:1] / 1024.0
        spread_now = padded[:, 1:2] / 1024.0 - middle * middle
        value = (convolved[...] - middle) * lax.rsqrt(spread_now + 1e-05)
        value = value * scale_ref[...] + shift_ref[...]
        conv_out[...] = (value * jax.nn.sigmoid(value)).astype(jnp.bfloat16)

    def mix(pieces, top_row, start):
        order = [lax.rem(group + hop, 4) for hop in range(4)]

        def columns(n, _):
            span = pl.ds(pl.multiple_of(512 * n, 512), 512)
            total = jnp.zeros((128, 512), jnp.float32) if start is None else start[:, span]
            for hop in range(4):
                rows = pl.ds(pl.multiple_of(top_row + 256 * order[hop], 256), 256)
                total = total + jnp.dot(
                    pieces[hop], out_w[rows, span], preferred_element_type=jnp.float32
                )
            if start is None:
                mixing[:, span] = total
            else:
                mixed_ref[:, span] = total.astype(jnp.bfloat16)
            return 0

        lax.fori_loop(0, 4, columns, 0)

    def advance(chunk, blocks, masked):
        states = [2 * chunk + head for head in range(2)]
        before = [tops[state] for state in states]
        sums = [totals[state] for state in states]
        scores = []
        for head in range(2):
            lanes = slice(128 * head, 128 * head + 128)
            keys = jnp.concatenate([kv[block, 0:256, lanes] for block in blocks], axis=0)
            scores.append(
                jnp.dot(keys, queries[states[head]], preferred_element_type=jnp.float32)
            )
        if masked:
            rows = len(blocks) * 256
            key_pos = lax.broadcasted_iota(jnp.int32, (rows, 512), 0) + 256 * blocks[0]
            query_pos = lax.broadcasted_iota(jnp.int32, (rows, 512), 1) & 255
            last = 2 * me + chunk * (63 - 4 * me)
            allowed = key_pos <= query_pos + 256 * last
            scores = [jnp.where(allowed, part, NEG) for part in scores]
        after = []
        for head in range(2):
            top = jnp.maximum(before[head], jnp.max(scores[head], axis=0, keepdims=True))
            weights = jnp.exp2(scores[head] - top)
            factor = jnp.exp2(before[head] - top)
            total = sums[head] * factor + jnp.sum(weights, axis=0, keepdims=True)
            shares = kv_values(blocks, head)
            added = jnp.dot(
                shares, weights.astype(jnp.bfloat16), preferred_element_type=jnp.float32
            )
            after.append((top, total, factor, added))
        for head in range(2):
            top, total, factor, added = after[head]
            tops[states[head]] = top
            totals[states[head]] = total
            summed[states[head]] = summed[states[head]] * factor + added

    def kv_values(blocks, head):
        rows = slice(256 + 128 * head, 384 + 128 * head)
        return jnp.concatenate([kv[block, rows, :] for block in blocks], axis=1)

    def work(ring, step):
        half, direction = ring // 2, ring % 2
        low = 4 * origin(half, direction, step) + half
        twin_copy(ring, step, 1 - core).wait_recv()
        for chunk in range(2):
            last = 2 * me + chunk * (63 - 4 * me)

            @pl.when(low + 2 < last)
            def _():
                advance(chunk, [low, low + 2], False)

            @pl.when(low + 2 >= last)
            def _():
                def item(j, _):
                    @pl.when(low + 2 * j <= last)
                    def _():
                        advance(chunk, [low + 2 * j], True)

                    return 0

                lax.fori_loop(0, 2, item, 0)

    def turn(t, _):
        step, part = t // 4 + 1, lax.rem(t, 4)
        for piece in range(SUBS // 4):
            sub = part * (SUBS // 4) + piece
            for ring in range(4):
                ring_arrival(ring, step, sub).wait_recv()

                @pl.when((step < 7) | (sub // (SUBS // 2) == ring % 2))
                def _():
                    ring_copy(ring, step + 1, sub).start()

        @pl.when(part == 3)
        def _():
            for ring in range(4):
                twin_copy(ring, step, core).start()

        @pl.when(t == 0)
        def _():
            for hop in range(1, 4):
                sums_copy(hop).start()

        @pl.when(t == 4)
        def _():
            normalize()

        @pl.when(t == 6)
        def _():
            for hop in range(1, 4):
                conv_copy(hop).start()
            mine = pl.ds(pl.multiple_of(128 * group, 128), 128)
            conv_in[0] = conv_out[mine, :]

        @pl.when(t == 12)
        def _():
            fetch.wait()
            for hop in range(1, 4):
                conv_copy(hop).wait_recv()
            mix(conv_in, 1024, None)

        @pl.when((step > 1) | (lax.rem(part, 2) == 0))
        def _():
            work(part, step - 1)

        return 0

    lax.fori_loop(0, 28, turn, 0)

    for half in range(2):
        for sub in range(SUBS):
            ring_arrival(2 * half + sub // (SUBS // 2), 8, sub).wait_recv()
        twin_copy(2 * half, 8, core).start()
    lax.fori_loop(0, 4, lambda r, _: (work(r, 7), 0)[1], 0)
    lax.fori_loop(0, 2, lambda h, _: (work(2 * h, 8), 0)[1], 0)

    logs_copy = pltpu.make_async_remote_copy(
        src_ref=logs_in.at[1], dst_ref=logs_in.at[2],
        send_sem=logs_sem.at[0], recv_sem=logs_sem.at[1],
        device_id={"sp": partner}, device_id_type=MESH,
    )

    def att_copy(part, target_sp, slot):
        return pltpu.make_async_remote_copy(
            src_ref=attended.at[part // 2, pl.ds(128 * (part % 2), 128)],
            dst_ref=attended_in.at[slot],
            send_sem=att_send.at[part], recv_sem=att_recv.at[slot],
            device_id={"sp": target_sp, "tp": part}, device_id_type=MESH,
        )

    for chunk in (1, 0):
        for head in range(2):
            state = 2 * chunk + head
            share = summed[state] / totals[state]
            out = share[:, 0:256] - lam_ref[head] * share[:, 256:512]
            power = jnp.mean(out * out, axis=0, keepdims=True)
            out = out * lax.rsqrt(power + 1e-06) * gain_ref[...]
            attended[chunk, :, 128 * head : 128 * head + 128] = out.T.astype(jnp.bfloat16)
            logs_in[chunk, head] = (tops[state] + jnp.log2(totals[state])) * (1.0 / LOG2E)

    for part in (2, 3):
        att_copy(part, partner, lax.rem(group + 4 - part, 4)).start()
    for part in (0, 1):

        @pl.when(group != part)
        def _():
            att_copy(part, me, lax.rem(group + 4 - part, 4)).start()

        @pl.when(group == part)
        def _():
            attended_in[0] = attended[0, 128 * part : 128 * part + 128, :]

    logs_copy.start()
    for slot in range(4):

        @pl.when((group >= 2) | (slot > 0))
        def _():
            att_copy(0, partner, slot).wait_recv()

    mix(attended_in, 0, mixing)

    logs_copy.wait()
    for head in range(2):
        for half in range(2):
            columns = slice(256 * half, 256 * half + 256)
            logs_ref[half, head : head + 1, 0:256] = logs_in[0, head, :, columns]
            logs_ref[half, head : head + 1, 256:512] = logs_in[2, head, :, columns]

    for part in (2, 3):
        att_copy(part, partner, lax.rem(group + 4 - part, 4)).wait_send()
    for part in (0, 1):

        @pl.when(group != part)
        def _():
            att_copy(part, me, lax.rem(group + 4 - part, 4)).wait_send()

    halo_copy.wait_send()
    for hop in range(1, 4):
        sums_copy(hop).wait_send()
        conv_copy(hop).wait_send()
    odd_copy.wait_send()
    for half in range(2):
        twin_copy(2 * half, 0, core).wait_send()
        twin_copy(2 * half, 8, core).wait_send()

    def drain(step, _):
        for ring in range(4):
            twin_copy(ring, step, core).wait_send()
            for sub in range(SUBS):
                ring_copy(ring, step, sub).wait_send()
        return 0

    lax.fori_loop(1, 8, drain, 0)
    for half in range(2):
        for sub in range(SUBS):
            ring_copy(2 * half + sub // (SUBS // 2), 8, sub).wait_send()


def attend(own, queries, gated, lam, gain, taps, scale, shift, out_w):
    vmem = pl.BlockSpec(memory_space=pltpu.VMEM)
    hbm = pl.BlockSpec(memory_space=pl.ANY)
    dma = pltpu.SemaphoreType.DMA
    return pl.pallas_call(
        attend_kernel,
        out_shape=(
            jax.ShapeDtypeStruct((128, 2048), jnp.bfloat16),
            jax.ShapeDtypeStruct((2, 2, 512), jnp.float32),
        ),
        in_specs=[hbm] + [vmem] * 7 + [hbm],
        out_specs=(vmem, vmem),
        scratch_shapes=[
            pltpu.VMEM((64, 512, 256), jnp.bfloat16),
            pltpu.VMEM((2, 128, 256), jnp.bfloat16),
            pltpu.VMEM((4, 128, 512), jnp.bfloat16),
            pltpu.VMEM((4, 1, 512), jnp.float32),
            pltpu.VMEM((4, 1, 512), jnp.float32),
            pltpu.VMEM((4, 128, 512), jnp.float32),
            pltpu.VMEM((32, 256), jnp.bfloat16),
            pltpu.VMEM((8, 544, 256), jnp.float32),
            pltpu.VMEM((512, 256), jnp.float32),
            pltpu.VMEM((4, 8, 512), jnp.float32),
            pltpu.VMEM((512, 256), jnp.bfloat16),
            pltpu.VMEM((4, 128, 256), jnp.bfloat16),
            pltpu.VMEM((2, 256, 256), jnp.bfloat16),
            pltpu.VMEM((4, 128, 256), jnp.bfloat16),
            pltpu.VMEM((3, 2, 1, 512), jnp.float32),
            pltpu.VMEM((2048, 2048), jnp.bfloat16),
            pltpu.VMEM((128, 2048), jnp.float32),
            dma((2,)), dma, dma, dma((4, 8, SUBS)), dma((4, 8, SUBS)), dma((4, 9)), dma((4, 9)),
            dma, dma((2,)), dma((4,)), dma((4,)), dma((4,)), dma((4,)), dma((4,)), dma((4,)), dma((2,)),
        ],
        compiler_params=pltpu.CompilerParams(
            collective_id=0, has_side_effects=True, vmem_limit_bytes=48 * 1024 * 1024
        ),
    )(own, queries, gated, lam, gain, taps, scale, shift, out_w)


def project_kernel(
    tok_ref, wq_ref, wk_ref, wv_ref, wa_ref, wg_ref, gain_ref, qk_ref, trig_ref,
    own_ref, query_ref, gated_ref,
    rows, weights, load_sem, weight_sem, send_sem, recv_sem, far_send, far_recv,
):
    me = lax.axis_index("tp")
    right, left = lax.rem(me + 1, 4), lax.rem(me + 3, 4)
    far = lax.rem(me + 2, 4)

    load = pltpu.make_async_copy(tok_ref, rows.at[me], load_sem)
    load.start()
    fetches = []
    for n, ref in enumerate((wq_ref, wk_ref, wv_ref, wa_ref, wg_ref)):
        fetches.append(
            pltpu.make_async_copy(ref, weights.at[:, pl.ds(256 * n, 256)], weight_sem.at[n])
        )
        fetches[-1].start()

    barrier = pltpu.get_barrier_semaphore()
    for peer in (left, right):
        pl.semaphore_signal(barrier, inc=1, device_id={"tp": peer}, device_id_type=MESH)
    load.wait()
    pl.semaphore_wait(barrier, 2)

    def hand(block, direction, half, send, recv):
        piece = rows.at[block, pl.ds(64 * half, 64)]
        return pltpu.make_async_remote_copy(
            src_ref=piece, dst_ref=piece, send_sem=send, recv_sem=recv,
            device_id={"tp": right if direction == 0 else left}, device_id_type=MESH,
        )

    def near(direction, half, block):
        return hand(
            block, direction, half, send_sem.at[direction, half], recv_sem.at[direction, half]
        )

    def beyond(direction, block):
        return hand(block, direction, direction, far_send.at[direction], far_recv.at[direction])

    for turn in range(2):
        near(0, turn, me).start()
        near(1, 1 - turn, me).start()

    def project(block):
        inputs = rows[block].astype(jnp.float32)
        power = jnp.mean(inputs * inputs, axis=-1, keepdims=True)
        normed = (inputs * lax.rsqrt(power + 1e-06) * gain_ref[...]).astype(jnp.bfloat16)
        places = pl.ds(pl.multiple_of(128 * block, 128), 128)
        pair, side = block // 2, pl.ds(pl.multiple_of(128 * lax.rem(block, 2), 128), 128)
        cosine, sine = trig_ref[0, :, places], trig_ref[1, :, places]

        def product(n):
            return jnp.dot(
                normed, weights[:, 256 * n : 256 * n + 256], preferred_element_type=jnp.float32
            ).astype(jnp.bfloat16).astype(jnp.float32)

        def prepared(flat, which):
            parts = []
            for group in range(4):
                piece = flat[64 * group : 64 * group + 64]
                power = jnp.mean(piece * piece, axis=0, keepdims=True)
                gains = qk_ref[which, 64 * group : 64 * group + 64]
                piece = piece * lax.rsqrt(power + 1e-06) * gains
                first, second = piece[:32], piece[32:]
                parts.append(first * cosine - second * sine)
                parts.append(second * cosine + first * sine)
            return jnp.concatenate(parts, axis=0)

        turned = prepared(product(0).T, 0).astype(jnp.bfloat16)
        for head in range(2):
            query_ref[pair, head, :, side] = turned[128 * head : 128 * head + 128]
        own_ref[pair, side, :] = prepared(product(1).T, 1).T.astype(jnp.bfloat16)
        own_ref[pair, 256:512, side] = product(2).T.astype(jnp.bfloat16)
        gated = product(3) * jax.nn.sigmoid(product(4))
        gated_ref[places, :] = gated.astype(jnp.bfloat16)

    for fetch in fetches:
        fetch.wait()

    def turn(n, _):
        block = lax.rem(me + n + n // 2 - 2 * (n // 3), 4)

        @pl.when(n == 1)
        def _():
            near(0, 0, left).wait_recv()
            beyond(0, left).start()
            near(1, 1, right).wait_recv()
            beyond(1, right).start()
            near(1, 0, right).wait_recv()

        @pl.when(n == 2)
        def _():
            near(0, 1, left).wait_recv()

        @pl.when(n == 3)
        def _():
            beyond(0, far).wait_recv()
            beyond(1, far).wait_recv()

        project(block)
        return 0

    lax.fori_loop(0, 4, turn, 0)

    for direction in range(2):
        for half in range(2):
            near(direction, half, me).wait_send()
        beyond(direction, left if direction == 0 else right).wait_send()


def project_all(tokens, matrices, norm_gain, qk, trig):
    vmem = pl.BlockSpec(memory_space=pltpu.VMEM)
    hbm = pl.BlockSpec(memory_space=pl.ANY)
    return pl.pallas_call(
        project_kernel,
        out_shape=(
            jax.ShapeDtypeStruct((2, 512, 256), jnp.bfloat16),
            jax.ShapeDtypeStruct((2, 2, 128, 256), jnp.bfloat16),
            jax.ShapeDtypeStruct((512, 256), jnp.bfloat16),
        ),
        in_specs=[hbm] * 6 + [vmem] * 3,
        out_specs=(vmem, vmem, vmem),
        scratch_shapes=[
            pltpu.VMEM((4, 128, 2048), jnp.bfloat16),
            pltpu.VMEM((2048, 1280), jnp.bfloat16),
            pltpu.SemaphoreType.DMA,
            pltpu.SemaphoreType.DMA((5,)),
            pltpu.SemaphoreType.DMA((2, 2)),
            pltpu.SemaphoreType.DMA((2, 2)),
            pltpu.SemaphoreType.DMA((2,)),
            pltpu.SemaphoreType.DMA((2,)),
        ],
        compiler_params=pltpu.CompilerParams(
            collective_id=1, has_side_effects=True, vmem_limit_bytes=32 * 1024 * 1024
        ),
    )(tokens, *matrices, norm_gain, qk, trig)


def per_device(
    tokens,
    norm_gain,
    query_weight,
    key_weight,
    value_weight,
    glu_value_weight,
    glu_gate_weight,
    qk_gain,
    mix_lambda,
    head_gain,
    conv_kernel,
    channel_gain,
    channel_shift,
    output_weight,
):
    offset = lax.axis_index("sp") * 512
    positions = (offset + jnp.arange(512, dtype=jnp.int32)).astype(jnp.float32)
    inverse = 10000.0 ** (-jnp.arange(0, 32, dtype=jnp.float32) * 2.0 / 64)
    angles = inverse[:, None] * positions[None, :]
    trig = jnp.stack([jnp.cos(angles), jnp.sin(angles)])
    gains = jnp.tile(qk_gain.reshape(128), 2)
    qk = jnp.stack([gains * (64 ** (-0.5) * LOG2E), gains])[:, :, None]
    matrices = (query_weight, key_weight, value_weight, glu_value_weight, glu_gate_weight)
    own, queries, gated = project_all(tokens, matrices, norm_gain[None, :], qk, trig)
    return attend(
        own, queries, gated, mix_lambda[:, None, None], head_gain[:, None], conv_kernel,
        channel_gain[None, :], channel_shift[None, :], output_weight,
    )


def solution(mesh):
    placed = (
        P(("sp", "tp"), None),
        P(),
        P(None, "tp"),
        P(None, "tp"),
        P(None, "tp"),
        P(None, "tp"),
        P(None, "tp"),
        P(),
        P("tp"),
        P(),
        P(None, "tp"),
        P("tp"),
        P("tp"),
        P(),
    )
    return jax.shard_map(
        per_device,
        mesh=mesh,
        in_specs=placed,
        out_specs=(P(("sp", "tp"), None), P(None, "tp", "sp")),
        check_vma=False,
    )
```

```python
import jax
import jax.numpy as jnp
from jax import lax
from jax.experimental import pallas as pl
from jax.experimental.pallas import tpu as pltpu
from jax.sharding import PartitionSpec as P

MESH = pl.DeviceIdType.MESH
LOG2E = 1.4426950408889634
NEG = -1e30
SUBS = 4
SUB_ROWS = 512 // SUBS


def place(half, chip_z, chip_y):
    total = lax.rem(chip_y + chip_z, 4)
    row = chip_y + half * (chip_z - chip_y)
    return row * 4 + total


def chip_at(half, position):
    row = position // 4
    other = lax.rem(lax.rem(position, 4) + 4 - row, 4)
    chip_y = row + half * (other - row)
    chip_z = other + half * (row - other)
    return chip_z * 4 + chip_y


def attend_kernel(
    own_ref, query_ref, gated_ref, lam_ref, gain_ref, taps_ref, scale_ref, shift_ref, out_w_ref,
    mixed_ref, logs_ref,
    kv, odd_in, queries, tops, totals, summed,
    halo, shifted, convolved, sums, conv_out, conv_in, attended, attended_in, logs_in, out_w, mixing,
    load_sem, odd_send, odd_recv, ring_send, ring_recv, twin_send, twin_recv,
    weight_sem, halo_sem, sums_send, sums_recv, conv_send, conv_recv, att_send, att_recv, logs_sem,
):
    me = lax.axis_index("sp")
    group = lax.axis_index("tp")
    core = lax.rem(me, 2)
    chip = me // 2
    chip_z, chip_y = chip // 4, lax.rem(chip, 4)
    twin = me + 1 - 2 * core
    partner = 31 - me

    def origin(half, direction, step):
        here = place(half, chip_z, chip_y)
        there = lax.rem(here + 16 - step + 2 * step * direction, 16)
        return chip_at(half, there)

    def onward(half, direction):
        here = place(half, chip_z, chip_y)
        there = lax.rem(here + 17 - 2 * direction, 16)
        return chip_at(half, there) * 2 + core

    def ring_copy(ring, step, sub):
        half, direction = ring // 2, ring % 2
        source = origin(half, direction, step - 1) * 2 + core
        piece = kv.at[2 * source + half, pl.ds(sub * SUB_ROWS, SUB_ROWS)]
        return pltpu.make_async_remote_copy(
            src_ref=piece, dst_ref=piece,
            send_sem=ring_send.at[ring, step - 1, sub],
            recv_sem=ring_recv.at[ring, step - 1, sub],
            device_id={"sp": onward(half, direction)}, device_id_type=MESH,
        )

    def ring_arrival(ring, step, sub):
        half, direction = ring // 2, ring % 2
        source = origin(half, direction, step) * 2 + core
        piece = kv.at[2 * source + half, pl.ds(sub * SUB_ROWS, SUB_ROWS)]
        return pltpu.make_async_remote_copy(
            src_ref=piece, dst_ref=piece,
            send_sem=ring_send.at[ring, step - 1, sub],
            recv_sem=ring_recv.at[ring, step - 1, sub],
            device_id={"sp": onward(half, direction)}, device_id_type=MESH,
        )

    def twin_copy(ring, step, sender):
        half, direction = ring // 2, ring % 2
        source = origin(half, direction, step) * 2 + sender
        piece = kv.at[2 * source + half]
        return pltpu.make_async_remote_copy(
            src_ref=piece, dst_ref=piece,
            send_sem=twin_send.at[ring, step],
            recv_sem=twin_recv.at[ring, step],
            device_id={"sp": twin}, device_id_type=MESH,
        )

    loads = []
    for half in range(2):
        loads.append(
            pltpu.make_async_copy(own_ref.at[half], kv.at[2 * me + half], load_sem.at[half])
        )
        loads[-1].start()

    fetch = pltpu.make_async_copy(out_w_ref, out_w, weight_sem)
    fetch.start()

    barrier = pltpu.get_barrier_semaphore()
    for ring in range(4):
        pl.semaphore_signal(
            barrier, inc=1, device_id={"sp": onward(ring // 2, ring % 2)}, device_id_type=MESH
        )
    pl.semaphore_signal(barrier, inc=1, device_id={"sp": twin}, device_id_type=MESH)
    after, before_me = lax.rem(me + 1, 32), lax.rem(me + 31, 32)
    for place_on_line in (after, before_me):
        pl.semaphore_signal(barrier, inc=1, device_id={"sp": place_on_line}, device_id_type=MESH)
    for hop in range(4):
        peer = lax.rem(group + hop, 4)
        pl.semaphore_signal(
            barrier, inc=1, device_id={"sp": partner, "tp": peer}, device_id_type=MESH
        )
        if hop > 0:
            pl.semaphore_signal(barrier, inc=1, device_id={"tp": peer}, device_id_type=MESH)

    for chunk in range(2):
        for head in range(2):
            tops[2 * chunk + head] = jnp.full((1, 512), NEG, jnp.float32)
            totals[2 * chunk + head] = jnp.zeros((1, 512), jnp.float32)
            summed[2 * chunk + head] = jnp.zeros((128, 512), jnp.float32)

    def spread(chunk, head, block):
        rows = lax.broadcasted_iota(jnp.int32, (128, 256), 0)
        zero = jnp.zeros((128, 256), jnp.bfloat16)
        queries[2 * chunk + head, :, 0:256] = jnp.where(rows < 64, block, zero)
        queries[2 * chunk + head, :, 256:512] = jnp.where(rows < 64, zero, block)

    for copy in loads:
        copy.wait()
    pl.semaphore_wait(barrier, 14)

    for sub in range(SUBS):
        for ring in range(4):
            ring_copy(ring, 1, sub).start()
    odd_copy = pltpu.make_async_remote_copy(
        src_ref=query_ref.at[1], dst_ref=odd_in, send_sem=odd_send, recv_sem=odd_recv,
        device_id={"sp": partner}, device_id_type=MESH,
    )
    odd_copy.start()
    halo_copy = pltpu.make_async_remote_copy(
        src_ref=gated_ref.at[pl.ds(480, 32)], dst_ref=halo,
        send_sem=halo_sem.at[0], recv_sem=halo_sem.at[1],
        device_id={"sp": after}, device_id_type=MESH,
    )
    halo_copy.start()
    for half in range(2):
        twin_copy(2 * half, 0, core).start()

    for head in range(2):
        spread(0, head, query_ref[0, head])

    def to_peers(source, target, send, recv, hop, rows=None):
        peer = lax.rem(group + hop, 4)
        piece = source if rows is None else source.at[pl.ds(pl.multiple_of(rows * peer, 16), rows)]
        return pltpu.make_async_remote_copy(
            src_ref=piece, dst_ref=target.at[4 - hop],
            send_sem=send.at[4 - hop], recv_sem=recv.at[4 - hop],
            device_id={"tp": peer}, device_id_type=MESH,
        )

    def sums_copy(hop):
        return to_peers(sums.at[0], sums, sums_send, sums_recv, hop)

    def conv_copy(hop):
        return to_peers(conv_out, conv_in, conv_send, conv_recv, hop, 128)

    def line_up():
        halo_copy.wait_recv()
        edge = halo[...].astype(jnp.float32)
        shifted[0, 0:32, :] = jnp.where(me == 0, jnp.zeros((32, 256), jnp.float32), edge)
        shifted[0, 32:544, :] = gated_ref[...].astype(jnp.float32)
        for shift in range(1, 8):
            shifted[shift, 0:536, :] = shifted[0, shift : shift + 536, :]

    def conv_tile(tile, _):
        base = tile * 32
        total = jnp.zeros((32, 256), jnp.float32)
        for tap in range(31):
            offset = tap + 2
            start = pl.multiple_of(base + offset // 8 * 8, 8)
            total = total + taps_ref[tap : tap + 1, :] * shifted[offset % 8, pl.ds(start, 32), :]
        convolved[pl.ds(pl.multiple_of(base, 32), 32), :] = total
        return 0

    def add_up():
        lanes = lax.broadcasted_iota(jnp.int32, (512, 128), 1)
        conv_now = convolved[...]
        plain = jnp.sum(conv_now, axis=1, keepdims=True)
        square = jnp.sum(conv_now * conv_now, axis=1, keepdims=True)
        both = jnp.where(lanes == 0, plain, jnp.where(lanes == 1, square, 0.0))
        sums[0] = both.T[0:8]

    def normalize():
        for hop in range(1, 4):
            sums_copy(hop).wait_recv()
        total = sums[0] + sums[1] + sums[2] + sums[3]
        padded = jnp.concatenate([total, jnp.zeros((120, 512), jnp.float32)], axis=0).T
        middle = padded[:, 0:1] / 1024.0
        spread_now = padded[:, 1:2] / 1024.0 - middle * middle
        value = (convolved[...] - middle) * lax.rsqrt(spread_now + 1e-05)
        value = value * scale_ref[...] + shift_ref[...]
        conv_out[...] = (value * jax.nn.sigmoid(value)).astype(jnp.bfloat16)

    def mix(pieces, top_row, start, first=0, count=4):
        order = [lax.rem(group + hop, 4) for hop in range(4)]

        def columns(n, _):
            span = pl.ds(pl.multiple_of(512 * n, 512), 512)
            total = jnp.zeros((128, 512), jnp.float32) if start is None else start[:, span]
            for hop in range(4):
                rows = pl.ds(pl.multiple_of(top_row + 256 * order[hop], 256), 256)
                total = total + jnp.dot(
                    pieces[hop], out_w[rows, span], preferred_element_type=jnp.float32
                )
            if start is None:
                mixing[:, span] = total
            else:
                mixed_ref[:, span] = total.astype(jnp.bfloat16)
            return 0

        lax.fori_loop(first, first + count, columns, 0)

    def advance(chunk, blocks, masked):
        states = [2 * chunk + head for head in range(2)]
        before = [tops[state] for state in states]
        sums = [totals[state] for state in states]
        scores = []
        for head in range(2):
            lanes = slice(128 * head, 128 * head + 128)
            keys = jnp.concatenate([kv[block, 0:256, lanes] for block in blocks], axis=0)
            scores.append(
                jnp.dot(keys, queries[states[head]], preferred_element_type=jnp.float32)
            )
        if masked:
            rows = len(blocks) * 256
            key_pos = lax.broadcasted_iota(jnp.int32, (rows, 512), 0) + 256 * blocks[0]
            query_pos = lax.broadcasted_iota(jnp.int32, (rows, 512), 1) & 255
            last = 2 * me + chunk * (63 - 4 * me)
            allowed = key_pos <= query_pos + 256 * last
            scores = [jnp.where(allowed, part, NEG) for part in scores]
        after = []
        for head in range(2):
            top = jnp.maximum(before[head], jnp.max(scores[head], axis=0, keepdims=True))
            weights = jnp.exp2(scores[head] - top)
            factor = jnp.exp2(before[head] - top)
            total = sums[head] * factor + jnp.sum(weights, axis=0, keepdims=True)
            shares = kv_values(blocks, head)
            added = jnp.dot(
                shares, weights.astype(jnp.bfloat16), preferred_element_type=jnp.float32
            )
            after.append((top, total, factor, added))
        for head in range(2):
            top, total, factor, added = after[head]
            tops[states[head]] = top
            totals[states[head]] = total
            summed[states[head]] = summed[states[head]] * factor + added

    def kv_values(blocks, head):
        rows = slice(256 + 128 * head, 384 + 128 * head)
        return jnp.concatenate([kv[block, rows, :] for block in blocks], axis=1)

    def work(half, step, chunk):
        last = 2 * me + chunk * (63 - 4 * me)
        ends = (step == 0) | (step == 8)
        lows = [4 * origin(half, direction, step) + half for direction in range(2)]
        fits = [low + 2 < last for low in lows]

        @pl.when(fits[0] & fits[1] & jnp.logical_not(ends))
        def _():
            advance(chunk, [lows[0], lows[0] + 2, lows[1], lows[1] + 2], False)

        @pl.when(jnp.logical_not(fits[0] & fits[1]) | ends)
        def _():
            def one_way(direction, _):
                low = lows[0] + direction * (lows[1] - lows[0])

                @pl.when(low + 2 < last)
                def _():
                    advance(chunk, [low, low + 2], False)

                @pl.when((low + 2 >= last) & (low <= last))
                def _():
                    def item(j, _):
                        @pl.when(low + 2 * j <= last)
                        def _():
                            advance(chunk, [low + 2 * j], True)

                        return 0

                    lax.fori_loop(0, 2, item, 0)

                return 0

            lax.fori_loop(0, jnp.where(ends, 1, 2), one_way, 0)

    def turn(t, _):
        step, part = t // 4 + 1, lax.rem(t, 4)

        @pl.when(step < 8)
        def _():
            for ring in range(4):
                ring_arrival(ring, step, part).wait_recv()

                @pl.when((step < 7) | (part // 2 == ring % 2))
                def _():
                    ring_copy(ring, step + 1, part).start()

        @pl.when(step == 8)
        def _():
            for half in range(2):
                ring_arrival(2 * half + part // 2, 8, part).wait_recv()

        @pl.when((part == 3) & (step < 9))
        def _():
            for ring in range(4):

                @pl.when((step < 8) | (ring % 2 == 0))
                def _():
                    twin_copy(ring, step, core).start()

        half, chunk = part // 2, lax.rem(part, 2)

        @pl.when(chunk == 0)
        def _():
            twin_copy(2 * half, step - 1, 1 - core).wait_recv()

            @pl.when((step > 1) & (step < 9))
            def _():
                twin_copy(2 * half + 1, step - 1, 1 - core).wait_recv()

        @pl.when(t == 0)
        def _():
            line_up()

        @pl.when(t == 1)
        def _():
            odd_copy.wait_recv()
            for head in range(2):
                spread(1, head, odd_in[head])

        work(half, step - 1, chunk)

        @pl.when((t >= 2) & (t < 10))
        def _():
            lax.fori_loop(2 * t - 4, 2 * t - 2, conv_tile, 0)

        @pl.when(t == 10)
        def _():
            add_up()

        @pl.when(t == 11)
        def _():
            for hop in range(1, 4):
                sums_copy(hop).start()

        @pl.when(t == 15)
        def _():
            normalize()

        @pl.when(t == 16)
        def _():
            for hop in range(1, 4):
                conv_copy(hop).start()
            mine = pl.ds(pl.multiple_of(128 * group, 128), 128)
            conv_in[0] = conv_out[mine, :]

        @pl.when(t == 20)
        def _():
            fetch.wait()
            for hop in range(1, 4):
                conv_copy(hop).wait_recv()

        @pl.when((t >= 20) & (t < 24))
        def _():
            mix(conv_in, 1024, None, t - 20, 1)

        return 0

    lax.fori_loop(0, 36, turn, 0)

    logs_copy = pltpu.make_async_remote_copy(
        src_ref=logs_in.at[1], dst_ref=logs_in.at[2],
        send_sem=logs_sem.at[0], recv_sem=logs_sem.at[1],
        device_id={"sp": partner}, device_id_type=MESH,
    )

    def att_copy(part, target_sp, slot):
        return pltpu.make_async_remote_copy(
            src_ref=attended.at[part // 2, pl.ds(128 * (part % 2), 128)],
            dst_ref=attended_in.at[slot],
            send_sem=att_send.at[part], recv_sem=att_recv.at[slot],
            device_id={"sp": target_sp, "tp": part}, device_id_type=MESH,
        )

    for chunk in (1, 0):
        for head in range(2):
            state = 2 * chunk + head
            share = summed[state] / totals[state]
            out = share[:, 0:256] - lam_ref[head] * share[:, 256:512]
            power = jnp.mean(out * out, axis=0, keepdims=True)
            out = (out * lax.rsqrt(power + 1e-06)).T * gain_ref[...]
            attended[chunk, :, 128 * head : 128 * head + 128] = out.astype(jnp.bfloat16)
            logs_in[chunk, head] = (tops[state] + jnp.log2(totals[state])) * (1.0 / LOG2E)

    for part in (2, 3):
        att_copy(part, partner, lax.rem(group + 4 - part, 4)).start()
    for part in (0, 1):

        @pl.when(group != part)
        def _():
            att_copy(part, me, lax.rem(group + 4 - part, 4)).start()

        @pl.when(group == part)
        def _():
            attended_in[0] = attended[0, 128 * part : 128 * part + 128, :]

    logs_copy.start()
    for slot in range(4):

        @pl.when((group >= 2) | (slot > 0))
        def _():
            att_copy(0, partner, slot).wait_recv()

    mix(attended_in, 0, mixing)

    logs_copy.wait()
    for head in range(2):
        for half in range(2):
            columns = slice(256 * half, 256 * half + 256)
            logs_ref[half, head : head + 1, 0:256] = logs_in[0, head, :, columns]
            logs_ref[half, head : head + 1, 256:512] = logs_in[2, head, :, columns]

    for part in (2, 3):
        att_copy(part, partner, lax.rem(group + 4 - part, 4)).wait_send()
    for part in (0, 1):

        @pl.when(group != part)
        def _():
            att_copy(part, me, lax.rem(group + 4 - part, 4)).wait_send()

    halo_copy.wait_send()
    for hop in range(1, 4):
        sums_copy(hop).wait_send()
        conv_copy(hop).wait_send()
    odd_copy.wait_send()
    for half in range(2):
        twin_copy(2 * half, 0, core).wait_send()
        twin_copy(2 * half, 8, core).wait_send()

    def drain(step, _):
        for ring in range(4):
            twin_copy(ring, step, core).wait_send()
            for sub in range(SUBS):
                ring_copy(ring, step, sub).wait_send()
        return 0

    lax.fori_loop(1, 8, drain, 0)
    for half in range(2):
        for sub in range(SUBS):
            ring_copy(2 * half + sub // (SUBS // 2), 8, sub).wait_send()


def attend(own, queries, gated, lam, gain, taps, scale, shift, out_w):
    vmem = pl.BlockSpec(memory_space=pltpu.VMEM)
    hbm = pl.BlockSpec(memory_space=pl.ANY)
    smem = pl.BlockSpec(memory_space=pltpu.SMEM)
    dma = pltpu.SemaphoreType.DMA
    return pl.pallas_call(
        attend_kernel,
        out_shape=(
            jax.ShapeDtypeStruct((128, 2048), jnp.bfloat16),
            jax.ShapeDtypeStruct((2, 2, 512), jnp.float32),
        ),
        in_specs=[hbm] + [vmem] * 2 + [smem] + [vmem] * 4 + [hbm],
        out_specs=(vmem, vmem),
        scratch_shapes=[
            pltpu.VMEM((64, 512, 256), jnp.bfloat16),
            pltpu.VMEM((2, 128, 256), jnp.bfloat16),
            pltpu.VMEM((4, 128, 512), jnp.bfloat16),
            pltpu.VMEM((4, 1, 512), jnp.float32),
            pltpu.VMEM((4, 1, 512), jnp.float32),
            pltpu.VMEM((4, 128, 512), jnp.float32),
            pltpu.VMEM((32, 256), jnp.bfloat16),
            pltpu.VMEM((8, 544, 256), jnp.float32),
            pltpu.VMEM((512, 256), jnp.float32),
            pltpu.VMEM((4, 8, 512), jnp.float32),
            pltpu.VMEM((512, 256), jnp.bfloat16),
            pltpu.VMEM((4, 128, 256), jnp.bfloat16),
            pltpu.VMEM((2, 256, 256), jnp.bfloat16),
            pltpu.VMEM((4, 128, 256), jnp.bfloat16),
            pltpu.VMEM((3, 2, 1, 512), jnp.float32),
            pltpu.VMEM((2048, 2048), jnp.bfloat16),
            pltpu.VMEM((128, 2048), jnp.float32),
            dma((2,)), dma, dma, dma((4, 8, SUBS)), dma((4, 8, SUBS)), dma((4, 9)), dma((4, 9)),
            dma, dma((2,)), dma((4,)), dma((4,)), dma((4,)), dma((4,)), dma((4,)), dma((4,)), dma((2,)),
        ],
        compiler_params=pltpu.CompilerParams(
            collective_id=0, has_side_effects=True, vmem_limit_bytes=67043328,
        ),
    )(own, queries, gated, lam, gain, taps, scale, shift, out_w)


def project_kernel(
    tok_ref, wq_ref, wk_ref, wv_ref, wa_ref, wg_ref, gain_ref, qk_ref, trig_ref,
    own_ref, query_ref, gated_ref,
    rows, weights, load_sem, weight_sem, send_sem, recv_sem, far_send, far_recv,
):
    me = lax.axis_index("tp")
    right, left = lax.rem(me + 1, 4), lax.rem(me + 3, 4)
    far = lax.rem(me + 2, 4)

    load = pltpu.make_async_copy(tok_ref, rows.at[me], load_sem)
    load.start()
    fetches = []
    for n, ref in enumerate((wq_ref, wk_ref, wv_ref, wa_ref, wg_ref)):
        fetches.append(
            pltpu.make_async_copy(ref, weights.at[:, pl.ds(256 * n, 256)], weight_sem.at[n])
        )
        fetches[-1].start()

    barrier = pltpu.get_barrier_semaphore()
    for peer in (left, right):
        pl.semaphore_signal(barrier, inc=1, device_id={"tp": peer}, device_id_type=MESH)
    load.wait()
    pl.semaphore_wait(barrier, 2)

    def hand(block, direction, half, send, recv):
        piece = rows.at[block, pl.ds(64 * half, 64)]
        return pltpu.make_async_remote_copy(
            src_ref=piece, dst_ref=piece, send_sem=send, recv_sem=recv,
            device_id={"tp": right if direction == 0 else left}, device_id_type=MESH,
        )

    def near(direction, half, block):
        return hand(
            block, direction, half, send_sem.at[direction, half], recv_sem.at[direction, half]
        )

    def beyond(direction, block):
        return hand(block, direction, direction, far_send.at[direction], far_recv.at[direction])

    for turn in range(2):
        near(0, turn, me).start()
        near(1, 1 - turn, me).start()

    def project(block):
        inputs = rows[block].astype(jnp.float32)
        power = jnp.mean(inputs * inputs, axis=-1, keepdims=True)
        normed = (inputs * lax.rsqrt(power + 1e-06) * gain_ref[...]).astype(jnp.bfloat16)
        places = pl.ds(pl.multiple_of(128 * block, 128), 128)
        pair, side = block // 2, pl.ds(pl.multiple_of(128 * lax.rem(block, 2), 128), 128)
        cosine, sine = trig_ref[0, :, places], trig_ref[1, :, places]

        def product(n):
            return jnp.dot(
                normed, weights[:, 256 * n : 256 * n + 256], preferred_element_type=jnp.float32
            ).astype(jnp.bfloat16).astype(jnp.float32)

        def prepared(flat, which):
            parts = []
            for group in range(4):
                piece = flat[64 * group : 64 * group + 64]
                power = jnp.mean(piece * piece, axis=0, keepdims=True)
                gains = columns[which][64 * (group % 2) : 64 * (group % 2) + 64]
                piece = piece * lax.rsqrt(power + 1e-06) * gains
                first, second = piece[:32], piece[32:]
                parts.append(first * cosine - second * sine)
                parts.append(second * cosine + first * sine)
            return jnp.concatenate(parts, axis=0)

        turned = prepared(product(0).T, 0).astype(jnp.bfloat16)
        for head in range(2):
            query_ref[pair, head, :, side] = turned[128 * head : 128 * head + 128]
        own_ref[pair, side, :] = prepared(product(1).T, 1).T.astype(jnp.bfloat16)
        own_ref[pair, 256:512, side] = product(2).T.astype(jnp.bfloat16)
        gated = product(3) * jax.nn.sigmoid(product(4))
        gated_ref[places, :] = gated.astype(jnp.bfloat16)

    for fetch in fetches:
        fetch.wait()

    line = jnp.concatenate([qk_ref[0:1], qk_ref[1:2]], axis=1)
    column = jnp.broadcast_to(line, (128, 128)).T[:, 0:1]
    columns = (column * (64 ** (-0.5) * LOG2E), column)

    def turn(n, _):
        block = lax.rem(me + n + n // 2 - 2 * (n // 3), 4)

        @pl.when(n == 1)
        def _():
            near(0, 0, left).wait_recv()
            beyond(0, left).start()
            near(1, 1, right).wait_recv()
            beyond(1, right).start()
            near(1, 0, right).wait_recv()

        @pl.when(n == 2)
        def _():
            near(0, 1, left).wait_recv()

        @pl.when(n == 3)
        def _():
            beyond(0, far).wait_recv()
            beyond(1, far).wait_recv()

        project(block)
        return 0

    lax.fori_loop(0, 4, turn, 0)

    for direction in range(2):
        for half in range(2):
            near(direction, half, me).wait_send()
        beyond(direction, left if direction == 0 else right).wait_send()


def project_all(tokens, matrices, norm_gain, qk, trig):
    vmem = pl.BlockSpec(memory_space=pltpu.VMEM)
    hbm = pl.BlockSpec(memory_space=pl.ANY)
    return pl.pallas_call(
        project_kernel,
        out_shape=(
            jax.ShapeDtypeStruct((2, 512, 256), jnp.bfloat16),
            jax.ShapeDtypeStruct((2, 2, 128, 256), jnp.bfloat16),
            jax.ShapeDtypeStruct((512, 256), jnp.bfloat16),
        ),
        in_specs=[hbm] * 6 + [vmem] * 3,
        out_specs=(vmem, vmem, vmem),
        scratch_shapes=[
            pltpu.VMEM((4, 128, 2048), jnp.bfloat16),
            pltpu.VMEM((2048, 1280), jnp.bfloat16),
            pltpu.SemaphoreType.DMA,
            pltpu.SemaphoreType.DMA((5,)),
            pltpu.SemaphoreType.DMA((2, 2)),
            pltpu.SemaphoreType.DMA((2, 2)),
            pltpu.SemaphoreType.DMA((2,)),
            pltpu.SemaphoreType.DMA((2,)),
        ],
        compiler_params=pltpu.CompilerParams(
            collective_id=1, has_side_effects=True, vmem_limit_bytes=67043328
        ),
    )(tokens, *matrices, norm_gain, qk, trig)


def per_device(
    tokens,
    norm_gain,
    query_weight,
    key_weight,
    value_weight,
    glu_value_weight,
    glu_gate_weight,
    qk_gain,
    mix_lambda,
    head_gain,
    conv_kernel,
    channel_gain,
    channel_shift,
    output_weight,
):
    offset = lax.axis_index("sp") * 512
    positions = (offset + jnp.arange(512, dtype=jnp.int32)).astype(jnp.float32)
    inverse = 10000.0 ** (-jnp.arange(0, 32, dtype=jnp.float32) * 2.0 / 64)
    angles = inverse[:, None] * positions[None, :]
    trig = jnp.stack([jnp.cos(angles), jnp.sin(angles)])
    matrices = (query_weight, key_weight, value_weight, glu_value_weight, glu_gate_weight)
    own, queries, gated = project_all(tokens, matrices, norm_gain[None, :], qk_gain, trig)
    return attend(
        own, queries, gated, mix_lambda, head_gain[None, :], conv_kernel,
        channel_gain[None, :], channel_shift[None, :], output_weight,
    )


def solution(mesh):
    placed = (
        P(("sp", "tp"), None),
        P(),
        P(None, "tp"),
        P(None, "tp"),
        P(None, "tp"),
        P(None, "tp"),
        P(None, "tp"),
        P(),
        P("tp"),
        P(),
        P(None, "tp"),
        P("tp"),
        P("tp"),
        P(),
    )
    return jax.shard_map(
        per_device,
        mesh=mesh,
        in_specs=placed,
        out_specs=(P(("sp", "tp"), None), P(None, "tp", "sp")),
        check_vma=False,
    )
```

```python
import jax
import jax.numpy as jnp
from jax import lax
from jax.experimental import pallas as pl
from jax.experimental.pallas import tpu as pltpu
from jax.sharding import PartitionSpec as P

MESH = pl.DeviceIdType.MESH
LOG2E = 1.4426950408889634
NEG = -1e30


def place(half, chip_z, chip_y):
    row = chip_z if half == 1 else chip_y
    return 4 * row + ((chip_y + chip_z) & 3)


def chip_at(half, position):
    row = position // 4
    other = (position + 12 - row) & 3
    return row * 4 + other if half == 1 else other * 4 + row


def layer_kernel(
    tok_ref, wq_ref, wk_ref, wv_ref, wa_ref, wg_ref, norm_ref, qk_ref, trig_ref,
    lam_ref, gain_ref, taps_ref, scale_ref, shift_ref, out_w_ref,
    mixed_ref, logs_ref,
    rows, weights, kv, odd, odd_in, queries, tops, totals, summed,
    gated, halo, shifted, convolved, sums, conv_out, conv_in, attended, attended_in, logs_in,
    out_w, mixing,
    load_sem, fetch_sem, near_send, near_recv, far_send, far_recv,
    odd_sem, ring_send, ring_recv, twin_send, twin_recv,
    weight_sem, halo_sem, sums_send, sums_recv, conv_send, conv_recv, att_send, att_recv, logs_sem,
):
    me = lax.axis_index("sp")
    group = lax.axis_index("tp")
    core = lax.rem(me, 2)
    chip = me // 2
    chip_z, chip_y = chip // 4, lax.rem(chip, 4)
    twin = me + 1 - 2 * core
    partner = 31 - me
    right, left, far = (lax.rem(group + hop, 4) for hop in (1, 3, 2))

    def block_of(unit):
        return lax.rem(group + unit + unit // 2 - 2 * (unit // 3), 4)

    def origin(half, direction, step):
        here = place(half, chip_z, chip_y)
        there = (here + 16 - step + 2 * step * direction) & 15
        return chip_at(half, there)

    def onward(half, direction):
        here = place(half, chip_z, chip_y)
        there = (here + 17 - 2 * direction) & 15
        return chip_at(half, there) * 2 + core

    ahead = [onward(ring // 2, ring % 2) for ring in range(4)]

    def ring_piece(ring, source_step, step, unit, span):
        half, direction = ring // 2, ring % 2
        source = origin(half, direction, source_step) * 2 + core
        piece = kv.at[half, source, unit]
        if span is not None:
            piece = kv.at[half, source, unit, pl.ds(128 * direction, 128)]
        return pltpu.make_async_remote_copy(
            src_ref=piece, dst_ref=piece,
            send_sem=ring_send.at[ring, step - 1, unit],
            recv_sem=ring_recv.at[ring, step - 1, unit],
            device_id={"sp": ahead[ring]}, device_id_type=MESH,
        )

    def ring_copy(ring, step, unit, span=None):
        return ring_piece(ring, step - 1, step, unit, span)

    def ring_arrival(ring, step, unit, span=None):
        return ring_piece(ring, step, step, unit, span)

    def twin_copy(ring, step, pair, sender):
        half, direction = ring // 2, ring % 2
        source = origin(half, direction, step) * 2 + sender
        piece = kv.at[half, source, pl.ds(2 * pair, 2)]
        return pltpu.make_async_remote_copy(
            src_ref=piece, dst_ref=piece,
            send_sem=twin_send.at[ring, step, pair], recv_sem=twin_recv.at[ring, step, pair],
            device_id={"sp": twin}, device_id_type=MESH,
        )

    def hand(block, direction, half, send, recv):
        piece = rows.at[block, pl.ds(64 * half, 64)]
        return pltpu.make_async_remote_copy(
            src_ref=piece, dst_ref=piece, send_sem=send, recv_sem=recv,
            device_id={"tp": right if direction == 0 else left}, device_id_type=MESH,
        )

    def near(direction, half, block):
        return hand(
            block, direction, half, near_send.at[direction, half], near_recv.at[direction, half]
        )

    def beyond(direction, block):
        return hand(block, direction, direction, far_send.at[direction], far_recv.at[direction])

    odd_copy = pltpu.make_async_remote_copy(
        src_ref=odd, dst_ref=odd_in, send_sem=odd_sem.at[0], recv_sem=odd_sem.at[1],
        device_id={"sp": partner}, device_id_type=MESH,
    )
    halo_copy = pltpu.make_async_remote_copy(
        src_ref=gated.at[pl.ds(480, 32)], dst_ref=halo,
        send_sem=halo_sem.at[0], recv_sem=halo_sem.at[1],
        device_id={"sp": lax.rem(me + 1, 32)}, device_id_type=MESH,
    )
    logs_copy = pltpu.make_async_remote_copy(
        src_ref=logs_in.at[1], dst_ref=logs_in.at[2],
        send_sem=logs_sem.at[0], recv_sem=logs_sem.at[1],
        device_id={"sp": partner}, device_id_type=MESH,
    )

    def to_peers(source, target, send, recv, hop, count=None):
        peer = lax.rem(group + hop, 4)
        piece = source
        if count is not None:
            piece = source.at[pl.ds(pl.multiple_of(count * peer, 16), count)]
        return pltpu.make_async_remote_copy(
            src_ref=piece, dst_ref=target.at[4 - hop],
            send_sem=send.at[4 - hop], recv_sem=recv.at[4 - hop],
            device_id={"tp": peer}, device_id_type=MESH,
        )

    def sums_copy(hop):
        return to_peers(sums.at[0], sums, sums_send, sums_recv, hop)

    def conv_copy(hop):
        return to_peers(conv_out, conv_in, conv_send, conv_recv, hop, 128)

    def att_copy(unit):
        hop = (0, 1, 3, 2)[unit]
        return pltpu.make_async_remote_copy(
            src_ref=attended.at[unit // 2, pl.ds(128 * (unit % 2), 128)],
            dst_ref=attended_in.at[4 - hop],
            send_sem=att_send.at[4 - hop], recv_sem=att_recv.at[4 - hop],
            device_id={"sp": me if unit < 2 else partner, "tp": lax.rem(group + hop, 4)},
            device_id_type=MESH,
        )

    load = pltpu.make_async_copy(tok_ref, rows.at[group], load_sem)
    load.start()
    fetches = []
    for n, ref in enumerate((wq_ref, wk_ref, wv_ref, wa_ref, wg_ref)):
        fetches.append(
            pltpu.make_async_copy(ref, weights.at[:, pl.ds(256 * n, 256)], fetch_sem.at[n])
        )
        fetches[-1].start()
    fetch = pltpu.make_async_copy(out_w_ref, out_w, weight_sem)

    barrier = pltpu.get_barrier_semaphore()
    for ring in range(4):
        pl.semaphore_signal(
            barrier, inc=1, device_id={"sp": onward(ring // 2, ring % 2)}, device_id_type=MESH
        )
    for other in (twin, lax.rem(me + 1, 32), lax.rem(me + 31, 32)):
        pl.semaphore_signal(barrier, inc=1, device_id={"sp": other}, device_id_type=MESH)
    for hop in range(4):
        peer = lax.rem(group + hop, 4)
        pl.semaphore_signal(
            barrier, inc=1, device_id={"sp": partner, "tp": peer}, device_id_type=MESH
        )
        if hop > 0:
            pl.semaphore_signal(barrier, inc=1, device_id={"tp": peer}, device_id_type=MESH)

    for state in range(4):
        tops[state] = jnp.full((1, 512), NEG, jnp.float32)
        totals[state] = jnp.zeros((1, 512), jnp.float32)
        summed[state] = jnp.zeros((128, 512), jnp.float32)
    line = jnp.concatenate([qk_ref[0:1], qk_ref[1:2]], axis=1)
    column = jnp.broadcast_to(line, (128, 128)).T[:, 0:1]

    load.wait()
    pl.semaphore_wait(barrier, 14)
    for turn_ in range(2):
        near(0, turn_, group).start()
        near(1, 1 - turn_, group).start()
    for copy in fetches:
        copy.wait()
    fetch.start()

    def spread(state, side, block):
        upper = lax.broadcasted_iota(jnp.int32, (128, 128), 0) < 64
        zero = jnp.zeros((128, 128), jnp.bfloat16)
        places = pl.multiple_of(128 * side, 128)
        queries[state, :, pl.ds(places, 128)] = jnp.where(upper, block, zero)
        queries[state, :, pl.ds(places + 256, 128)] = jnp.where(upper, zero, block)

    def project(unit):
        block = block_of(unit)
        inputs = rows[block].astype(jnp.float32)
        power = jnp.mean(inputs * inputs, axis=-1, keepdims=True)
        normed = (inputs * lax.rsqrt(power + 1e-06) * norm_ref[...]).astype(jnp.bfloat16)
        places = pl.ds(pl.multiple_of(128 * block, 128), 128)
        cosine, sine = trig_ref[0, :, places], trig_ref[1, :, places]

        def product(n):
            return jnp.dot(
                normed, weights[:, 256 * n : 256 * n + 256], preferred_element_type=jnp.float32
            ).astype(jnp.bfloat16).astype(jnp.float32)

        def prepared(flat, gains):
            parts = []
            for part in range(4):
                piece = flat[64 * part : 64 * part + 64]
                power = jnp.mean(piece * piece, axis=0, keepdims=True)
                piece = piece * lax.rsqrt(power + 1e-06)
                piece = piece * gains[64 * (part % 2) : 64 * (part % 2) + 64]
                first, second = piece[:32], piece[32:]
                parts.append(first * cosine - second * sine)
                parts.append(second * cosine + first * sine)
            return jnp.concatenate(parts, axis=0)

        keys = prepared(product(1).T, column).T.astype(jnp.bfloat16)
        values = product(2).T.astype(jnp.bfloat16)
        for head in range(2):
            part = slice(128 * head, 128 * head + 128)
            kv[head, me, unit, 0:128, :] = keys[:, part]
            kv[head, me, unit, 128:256, :] = values[part, :]
        turned = prepared(product(0).T, column * (64 ** (-0.5) * LOG2E)).astype(jnp.bfloat16)

        @pl.when(unit < 2)
        def _():
            for head in range(2):
                spread(head, unit, turned[128 * head : 128 * head + 128])

        @pl.when(unit >= 2)
        def _():
            for head in range(2):
                odd[unit - 2, head] = turned[128 * head : 128 * head + 128]

        gate = (product(3) * jax.nn.sigmoid(product(4))).astype(jnp.bfloat16)
        gated[places, :] = gate
        start = pl.multiple_of(128 * block + 32, 32)
        shifted[0, pl.ds(start, 128), :] = gate.astype(jnp.float32)
        for ring in range(4):
            ring_copy(ring, 1, unit).start()

        @pl.when((unit & 1) == 1)
        def _():
            for half in range(2):
                twin_copy(2 * half, 0, unit // 2, core).start()

    def advance(half, owner, chunk, masked):
        state = 2 * chunk + half
        spans = [(2 * owner + side, unit) for side in range(2) for unit in range(4)]
        keys = jnp.concatenate([kv[half, dev, unit, 0:128, :] for dev, unit in spans], axis=0)
        values = jnp.concatenate([kv[half, dev, unit, 128:256, :] for dev, unit in spans], axis=1)
        if masked:
            across = lax.broadcasted_iota(jnp.int32, (128, 256), 1)
            down = lax.broadcasted_iota(jnp.int32, (128, 256), 0)
            block = jnp.where(across < 128, block_of(2 * chunk), block_of(2 * chunk + 1))
            target = me + chunk * (31 - 2 * me)
            query_pos = 512 * target + 128 * block + (across & 127)
            allowed = jnp.concatenate(
                [down + 512 * dev + 128 * block_of(unit) <= query_pos for dev, unit in spans], axis=0
            )
        before = [tops[state, :, 256 * m : 256 * m + 256] for m in range(2)]
        sums_before = [totals[state, :, 256 * m : 256 * m + 256] for m in range(2)]
        scores = []
        for m in range(2):
            part = jnp.dot(
                keys, queries[state, :, 256 * m : 256 * m + 256], preferred_element_type=jnp.float32
            )
            scores.append(jnp.where(allowed, part, 3.0 * NEG) if masked else part)
        after = []
        for m in range(2):
            top = jnp.maximum(before[m], jnp.max(scores[m], axis=0, keepdims=True))
            shares = jnp.exp2(scores[m] - top)
            factor = jnp.exp2(before[m] - top)
            total = sums_before[m] * factor + jnp.sum(shares, axis=0, keepdims=True)
            added = jnp.dot(
                values, shares.astype(jnp.bfloat16), preferred_element_type=jnp.float32
            )
            after.append((top, total, factor, added))
        for m in range(2):
            top, total, factor, added = after[m]
            columns = slice(256 * m, 256 * m + 256)
            tops[state, :, columns] = top
            totals[state, :, columns] = total
            summed[state, :, columns] = summed[state, :, columns] * factor + added

    def target_of(chunk):
        return (me + chunk * (31 - 2 * me)) // 2

    def wanted(half, turned, step):
        owner = origin(half, turned // 2, step)
        return (owner <= target_of(1 - (turned & 1))).astype(jnp.int32)

    def compute(pending, done):
        low = pending & (-pending)
        index = jnp.int32(0)
        for size, mask in ((1, 0xAAAAAA), (2, 0xCCCCCC), (4, 0xF0F0F0), (8, 0xFF00), (16, 0xFF0000)):
            index = index + size * ((low & mask) != 0).astype(jnp.int32)
        step = done - 2 + index // 8
        turned, half = (index & 7) // 2, index & 1
        chunk = 1 - (turned & 1)
        direction = turned // 2
        owners = [origin(n, direction, step) for n in range(2)]
        owner = owners[0] + half * (owners[1] - owners[0])

        @pl.when(owner < target_of(chunk))
        def _():
            advance(half, owner, chunk, False)

        @pl.when(owner == target_of(chunk))
        def _():
            advance(half, owner, chunk, True)

        return pending & (pending - 1)

    def line_up():
        halo_copy.wait_recv()
        edge = halo[...].astype(jnp.float32)
        shifted[0, 0:32, :] = jnp.where(me == 0, jnp.zeros((32, 256), jnp.float32), edge)

    def line_up_by(shift):
        shifted[shift, 0:536, :] = shifted[0, shift : shift + 536, :]

    def conv_tile(tile, _):
        base = tile * 32
        total = jnp.zeros((32, 256), jnp.float32)
        for tap in range(31):
            offset = tap + 2
            start = pl.multiple_of(base + offset // 8 * 8, 8)
            total = total + taps_ref[tap : tap + 1, :] * shifted[offset % 8, pl.ds(start, 32), :]
        convolved[pl.ds(pl.multiple_of(base, 32), 32), :] = total
        return 0

    def add_up():
        lanes = lax.broadcasted_iota(jnp.int32, (512, 128), 1)
        conv_now = convolved[...]
        plain = jnp.sum(conv_now, axis=1, keepdims=True)
        square = jnp.sum(conv_now * conv_now, axis=1, keepdims=True)
        both = jnp.where(lanes == 0, plain, jnp.where(lanes == 1, square, 0.0))
        sums[0] = both.T[0:8]

    def normalize():
        for hop in range(1, 4):
            sums_copy(hop).wait_recv()
        total = sums[0] + sums[1] + sums[2] + sums[3]
        padded = jnp.concatenate([total, jnp.zeros((120, 512), jnp.float32)], axis=0).T
        middle = padded[:, 0:1] / 1024.0
        spread_now = padded[:, 1:2] / 1024.0 - middle * middle
        value = (convolved[...] - middle) * lax.rsqrt(spread_now + 1e-05)
        value = value * scale_ref[...] + shift_ref[...]
        conv_out[...] = (value * jax.nn.sigmoid(value)).astype(jnp.bfloat16)

    def mix(pieces, top_row, start, first=0, count=4):
        order = [lax.rem(group + hop, 4) for hop in range(4)]

        def columns(n, _):
            span = pl.ds(pl.multiple_of(512 * n, 512), 512)
            total = jnp.zeros((128, 512), jnp.float32) if start is None else start[:, span]
            for hop in range(4):
                rows = pl.ds(pl.multiple_of(top_row + 256 * order[hop], 256), 256)
                total = total + jnp.dot(
                    pieces[hop], out_w[rows, span], preferred_element_type=jnp.float32
                )
            if start is None:
                mixing[:, span] = total
            else:
                mixed_ref[:, span] = total.astype(jnp.bfloat16)
            return 0

        lax.fori_loop(first, first + count, columns, 0)

    def turn(t, pending):
        lap, unit = t // 4 + 1, lax.rem(t, 4)
        step = lap - jnp.where(unit == 0, 0, jnp.where(unit == 3, 1, 1))
        done = lap - 2

        @pl.when(t == 1)
        def _():
            near(0, 0, left).wait_recv()
            beyond(0, left).start()
            near(1, 1, right).wait_recv()
            beyond(1, right).start()

        @pl.when(t == 4)
        def _():
            near(1, 0, right).wait_recv()

        @pl.when(t == 5)
        def _():
            near(0, 1, left).wait_recv()

        @pl.when(t == 6)
        def _():
            beyond(0, far).wait_recv()
            beyond(1, far).wait_recv()

        @pl.when((t == 0) | (t == 4) | (t == 5) | (t == 6))
        def _():
            project(jnp.where(t == 0, 0, jnp.where(t == 6, 3, t - 3)))

        @pl.when(t == 6)
        def _():
            odd_copy.start()
            halo_copy.start()

        @pl.when((step >= 1) & (step < 8))
        def _():
            for ring in range(4):
                half, direction = ring // 2, ring % 2
                source = origin(half, direction, step) * 2 + core
                piece = kv.at[half, source, unit]
                pltpu.make_async_remote_copy(
                    src_ref=piece, dst_ref=piece,
                    send_sem=ring_send.at[ring, step - 1, unit],
                    recv_sem=ring_recv.at[ring, step - 1, unit],
                    device_id={"sp": ahead[ring]}, device_id_type=MESH,
                ).wait_recv()

                @pl.when(step < 7)
                def _():
                    pltpu.make_async_remote_copy(
                        src_ref=piece, dst_ref=piece,
                        send_sem=ring_send.at[ring, step, unit],
                        recv_sem=ring_recv.at[ring, step, unit],
                        device_id={"sp": ahead[ring]}, device_id_type=MESH,
                    ).start()

                @pl.when(step == 7)
                def _():
                    share = kv.at[half, source, unit, pl.ds(128 * direction, 128)]
                    pltpu.make_async_remote_copy(
                        src_ref=share, dst_ref=share,
                        send_sem=ring_send.at[ring, 7, unit], recv_sem=ring_recv.at[ring, 7, unit],
                        device_id={"sp": ahead[ring]}, device_id_type=MESH,
                    ).start()

            @pl.when((unit & 1) == 1)
            def _():
                for ring in (0, 2, 1, 3):
                    twin_copy(ring, step, unit // 2, core).start()

        @pl.when(step == 8)
        def _():
            for half in range(2):
                for direction in range(2):
                    ring_arrival(2 * half + direction, 8, unit, True).wait_recv()

                @pl.when((unit & 1) == 1)
                def _():
                    twin_copy(2 * half, 8, unit // 2, core).start()

        @pl.when(t == 8)
        def _():
            odd_copy.wait_recv()
            for side in range(2):
                for head in range(2):
                    spread(2 + head, side, odd_in[side, head])

            for half in range(2):
                for pair in range(2):
                    twin_copy(2 * half, 0, pair, 1 - core).wait_recv()

        for direction in range(2):

            @pl.when((done >= 1) & (unit == 2 * direction) & ((done < 8) | (direction == 0)))
            def _():
                for half in range(2):
                    for pair in range(2):
                        twin_copy(2 * half + direction, done, pair, 1 - core).wait_recv()

        pending = jnp.where(unit == 0, pending // 256, pending)
        for half in range(2):
            for turned in range(2):
                bit = 1 << (8 + 2 * turned + half)
                pending = pending + jnp.where(t == 8, bit * wanted(half, turned, 0), 0)
            valid = (done >= 1) & ((done < 8) | (unit < 2)) & (done <= 8)
            bit = jnp.where(unit == 0, 1, jnp.where(unit == 1, 4, jnp.where(unit == 2, 16, 64)))
            bit = bit * (65536 << half)
            step_now = jnp.clip(done, 0, 8)
            pending = pending + jnp.where(valid, bit * wanted(half, unit, step_now), 0)
        count = (pending != 0).astype(jnp.int32) + (
            ((pending & 255) != 0) & ((pending & (pending - 1)) != 0)
        ).astype(jnp.int32)
        pending = lax.fori_loop(0, count, lambda n, bits: compute(bits, done), pending)

        @pl.when(t == 9)
        def _():
            line_up()

        for shift in range(1, 8):

            @pl.when(t == 9 + (shift + 1) // 2)
            def _():
                line_up_by(shift)

        @pl.when((t >= 14) & (t < 22))
        def _():
            lax.fori_loop(2 * t - 28, 2 * t - 26, conv_tile, 0)

        @pl.when(t == 22)
        def _():
            add_up()

        @pl.when(t == 23)
        def _():
            for hop in range(1, 4):
                sums_copy(hop).start()

        @pl.when(t == 28)
        def _():
            normalize()

        @pl.when(t == 29)
        def _():
            for hop in range(1, 4):
                conv_copy(hop).start()
            mine = pl.ds(pl.multiple_of(128 * group, 128), 128)
            conv_in[0] = conv_out[mine, :]

        @pl.when(t == 34)
        def _():
            fetch.wait()
            for hop in range(1, 4):
                conv_copy(hop).wait_recv()

        @pl.when((t >= 34) & (t < 38))
        def _():
            mix(conv_in, 1024, None, t - 34, 1)

        return pending

    pending = lax.fori_loop(0, 40, turn, jnp.int32(0))

    def finish(chunk):
        for half in range(2):
            state = 2 * chunk + half
            share = summed[state] / totals[state]
            out = share[:, 0:256] - lam_ref[half] * share[:, 256:512]
            power = jnp.mean(out * out, axis=0, keepdims=True)
            out = (out * lax.rsqrt(power + 1e-06)).T * gain_ref[...]
            attended[chunk, :, 128 * half : 128 * half + 128] = out.astype(jnp.bfloat16)
            logs_in[chunk, half] = (tops[state] + jnp.log2(totals[state])) * (1.0 / LOG2E)

    def clear(bits):
        count = jnp.int32(0)
        for n in range(24):
            count = count + ((bits & (1 << n)) != 0).astype(jnp.int32)
        lax.fori_loop(0, count, lambda n, left: compute(left, 8), bits)

    clear(pending & 0x333333)
    finish(1)
    att_copy(3).start()
    att_copy(2).start()
    logs_copy.start()
    clear(pending & 0xCCCCCC)
    finish(0)
    att_copy(1).start()
    attended_in[0] = attended[0, 0:128, :]

    halo_copy.wait_send()
    odd_copy.wait_send()
    for hop in range(1, 4):
        sums_copy(hop).wait_send()
        conv_copy(hop).wait_send()
    for direction in range(2):
        for half in range(2):
            near(direction, half, group).wait_send()
        beyond(direction, left if direction == 0 else right).wait_send()

    def drain(step, _):
        for ring in range(4):
            for unit in range(4):
                ring_copy(ring, step, unit).wait_send()
            for pair in range(2):
                twin_copy(ring, step, pair, core).wait_send()
        return 0

    lax.fori_loop(1, 8, drain, 0)
    for half in range(2):
        for pair in range(2):
            twin_copy(2 * half, 0, pair, core).wait_send()
            twin_copy(2 * half, 8, pair, core).wait_send()
    for unit in range(4):
        for ring in range(4):
            ring_copy(ring, 8, unit, True).wait_send()
    logs_copy.wait()
    for unit in range(4):
        places = pl.ds(pl.multiple_of(128 * block_of(unit), 128), 128)
        for half in range(2):
            for m in range(2):
                start = 256 * m + 128 * (unit % 2)
                logs_ref[m, half : half + 1, places] = logs_in[
                    2 * (unit // 2), half, :, start : start + 128
                ]

    for unit in (1, 2, 3):
        att_copy(unit).wait_recv()
    mix(attended_in, 0, mixing)
    for unit in (1, 2, 3):
        att_copy(unit).wait_send()


def layer(*operands):
    vmem = pl.BlockSpec(memory_space=pltpu.VMEM)
    hbm = pl.BlockSpec(memory_space=pl.ANY)
    smem = pl.BlockSpec(memory_space=pltpu.SMEM)
    dma = pltpu.SemaphoreType.DMA
    bf16, f32 = jnp.bfloat16, jnp.float32
    return pl.pallas_call(
        layer_kernel,
        out_shape=(
            jax.ShapeDtypeStruct((128, 2048), bf16),
            jax.ShapeDtypeStruct((2, 2, 512), f32),
        ),
        in_specs=[hbm] * 6 + [vmem] * 3 + [smem] + [vmem] * 4 + [hbm],
        out_specs=(vmem, vmem),
        scratch_shapes=[
            pltpu.VMEM((4, 128, 2048), bf16),
            pltpu.VMEM((2048, 1280), bf16),
            pltpu.VMEM((2, 32, 4, 256, 128), bf16),
            pltpu.VMEM((2, 2, 128, 128), bf16),
            pltpu.VMEM((2, 2, 128, 128), bf16),
            pltpu.VMEM((4, 128, 512), bf16),
            pltpu.VMEM((4, 1, 512), f32),
            pltpu.VMEM((4, 1, 512), f32),
            pltpu.VMEM((4, 128, 512), f32),
            pltpu.VMEM((512, 256), bf16),
            pltpu.VMEM((32, 256), bf16),
            pltpu.VMEM((8, 544, 256), f32),
            pltpu.VMEM((512, 256), f32),
            pltpu.VMEM((4, 8, 512), f32),
            pltpu.VMEM((512, 256), bf16),
            pltpu.VMEM((4, 128, 256), bf16),
            pltpu.VMEM((2, 256, 256), bf16),
            pltpu.VMEM((4, 128, 256), bf16),
            pltpu.VMEM((3, 2, 1, 512), f32),
            pltpu.VMEM((2048, 2048), bf16),
            pltpu.VMEM((128, 2048), f32),
            dma, dma((5,)), dma((2, 2)), dma((2, 2)), dma((2,)), dma((2,)),
            dma((2,)), dma((4, 8, 4)), dma((4, 8, 4)), dma((4, 9, 2)), dma((4, 9, 2)),
            dma, dma((2,)), dma((4,)), dma((4,)), dma((4,)), dma((4,)), dma((4,)), dma((4,)), dma((2,)),
        ],
        compiler_params=pltpu.CompilerParams(
            collective_id=0, has_side_effects=True, vmem_limit_bytes=67043328,
        ),
    )(*operands)


def per_device(
    tokens,
    norm_gain,
    query_weight,
    key_weight,
    value_weight,
    glu_value_weight,
    glu_gate_weight,
    qk_gain,
    mix_lambda,
    head_gain,
    conv_kernel,
    channel_gain,
    channel_shift,
    output_weight,
):
    offset = lax.axis_index("sp") * 512
    positions = (offset + jnp.arange(512, dtype=jnp.int32)).astype(jnp.float32)
    inverse = 10000.0 ** (-jnp.arange(0, 32, dtype=jnp.float32) * 2.0 / 64)
    angles = inverse[:, None] * positions[None, :]
    trig = jnp.stack([jnp.cos(angles), jnp.sin(angles)])
    return layer(
        tokens, query_weight, key_weight, value_weight, glu_value_weight, glu_gate_weight,
        norm_gain[None, :], qk_gain, trig, mix_lambda, head_gain[None, :], conv_kernel,
        channel_gain[None, :], channel_shift[None, :], output_weight,
    )


def solution(mesh):
    placed = (
        P(("sp", "tp"), None),
        P(),
        P(None, "tp"),
        P(None, "tp"),
        P(None, "tp"),
        P(None, "tp"),
        P(None, "tp"),
        P(),
        P("tp"),
        P(),
        P(None, "tp"),
        P("tp"),
        P("tp"),
        P(),
    )
    return jax.shard_map(
        per_device,
        mesh=mesh,
        in_specs=placed,
        out_specs=(P(("sp", "tp"), None), P(None, "tp", "sp")),
        check_vma=False,
    )
```

```python
import jax
import jax.numpy as jnp
from jax import lax
from jax.experimental import pallas as pl
from jax.experimental.pallas import tpu as pltpu
from jax.sharding import PartitionSpec as P

MESH = pl.DeviceIdType.MESH
LOG2E = 1.4426950408889634
NEG = -1e30


def place(half, chip_z, chip_y):
    row = chip_z if half == 1 else chip_y
    return 4 * row + ((chip_y + chip_z) & 3)


def chip_at(half, position):
    row = position // 4
    other = (position + 12 - row) & 3
    return row * 4 + other if half == 1 else other * 4 + row


def layer_kernel(
    tok_ref, wq_ref, wk_ref, wv_ref, wa_ref, wg_ref, norm_ref, qk_ref, cosine_ref, sine_ref,
    lam_ref, gain_ref, taps_ref, scale_ref, shift_ref, out_w_ref,
    mixed_ref, logs_ref,
    rows, weights, kv, odd, odd_in, queries, tops, totals, summed,
    gated, halo, shifted, convolved, sums, conv_out, conv_in, attended, attended_in, logs_in,
    out_w, mixing,
    load_sem, fetch_sem, near_send, near_recv, far_send, far_recv,
    odd_sem, ring_send, ring_recv, twin_send, twin_recv,
    weight_sem, halo_sem, sums_send, sums_recv, conv_send, conv_recv, att_send, att_recv, logs_sem,
):
    me = lax.axis_index("sp")
    group = lax.axis_index("tp")
    core = lax.rem(me, 2)
    chip = me // 2
    chip_z, chip_y = chip // 4, lax.rem(chip, 4)
    twin = me + 1 - 2 * core
    partner = 31 - me
    right, left, far = (lax.rem(group + hop, 4) for hop in (1, 3, 2))

    def block_of(unit):
        return lax.rem(group + unit + unit // 2 - 2 * (unit // 3), 4)

    def origin(half, direction, step):
        here = place(half, chip_z, chip_y)
        there = (here + 16 - step + 2 * step * direction) & 15
        return chip_at(half, there)

    def onward(half, direction):
        here = place(half, chip_z, chip_y)
        there = (here + 17 - 2 * direction) & 15
        return chip_at(half, there) * 2 + core

    ahead = [onward(ring // 2, ring % 2) for ring in range(4)]

    def ring_piece(ring, source_step, step, unit, span):
        half, direction = ring // 2, ring % 2
        source = origin(half, direction, source_step) * 2 + core
        piece = kv.at[half, source, unit]
        if span is not None:
            piece = kv.at[half, source, unit, pl.ds(128 * direction, 128)]
        return pltpu.make_async_remote_copy(
            src_ref=piece, dst_ref=piece,
            send_sem=ring_send.at[ring, step - 1, unit],
            recv_sem=ring_recv.at[ring, step - 1, unit],
            device_id={"sp": ahead[ring]}, device_id_type=MESH,
        )

    def ring_copy(ring, step, unit, span=None):
        return ring_piece(ring, step - 1, step, unit, span)

    def ring_arrival(ring, step, unit, span=None):
        return ring_piece(ring, step, step, unit, span)

    def twin_copy(ring, step, pair, sender):
        half, direction = ring // 2, ring % 2
        source = origin(half, direction, step) * 2 + sender
        piece = kv.at[half, source, pl.ds(2 * pair, 2)]
        return pltpu.make_async_remote_copy(
            src_ref=piece, dst_ref=piece,
            send_sem=twin_send.at[ring, step, pair], recv_sem=twin_recv.at[ring, step, pair],
            device_id={"sp": twin}, device_id_type=MESH,
        )

    def hand(block, direction, half, send, recv):
        piece = rows.at[block, pl.ds(64 * half, 64)]
        return pltpu.make_async_remote_copy(
            src_ref=piece, dst_ref=piece, send_sem=send, recv_sem=recv,
            device_id={"tp": right if direction == 0 else left}, device_id_type=MESH,
        )

    def near(direction, half, block):
        return hand(
            block, direction, half, near_send.at[direction, half], near_recv.at[direction, half]
        )

    def beyond(direction, block):
        return hand(block, direction, direction, far_send.at[direction], far_recv.at[direction])

    odd_copy = pltpu.make_async_remote_copy(
        src_ref=odd, dst_ref=odd_in, send_sem=odd_sem.at[0], recv_sem=odd_sem.at[1],
        device_id={"sp": partner}, device_id_type=MESH,
    )
    halo_copy = pltpu.make_async_remote_copy(
        src_ref=gated.at[pl.ds(480, 32)], dst_ref=halo,
        send_sem=halo_sem.at[0], recv_sem=halo_sem.at[1],
        device_id={"sp": lax.rem(me + 1, 32)}, device_id_type=MESH,
    )
    logs_copy = pltpu.make_async_remote_copy(
        src_ref=logs_in.at[1], dst_ref=logs_in.at[2],
        send_sem=logs_sem.at[0], recv_sem=logs_sem.at[1],
        device_id={"sp": partner}, device_id_type=MESH,
    )

    def to_peers(source, target, send, recv, hop, count=None):
        peer = lax.rem(group + hop, 4)
        piece = source
        if count is not None:
            piece = source.at[pl.ds(pl.multiple_of(count * peer, 16), count)]
        return pltpu.make_async_remote_copy(
            src_ref=piece, dst_ref=target.at[4 - hop],
            send_sem=send.at[4 - hop], recv_sem=recv.at[4 - hop],
            device_id={"tp": peer}, device_id_type=MESH,
        )

    def sums_copy(hop):
        return to_peers(sums.at[0], sums, sums_send, sums_recv, hop)

    def conv_copy(hop):
        return to_peers(conv_out, conv_in, conv_send, conv_recv, hop, 128)

    def att_copy(unit):
        hop = (0, 1, 3, 2)[unit]
        return pltpu.make_async_remote_copy(
            src_ref=attended.at[unit // 2, pl.ds(128 * (unit % 2), 128)],
            dst_ref=attended_in.at[4 - hop],
            send_sem=att_send.at[4 - hop], recv_sem=att_recv.at[4 - hop],
            device_id={"sp": me if unit < 2 else partner, "tp": lax.rem(group + hop, 4)},
            device_id_type=MESH,
        )

    load = pltpu.make_async_copy(tok_ref, rows.at[group], load_sem)
    load.start()
    fetches = []
    for n, ref in enumerate((wq_ref, wk_ref, wv_ref, wa_ref, wg_ref)):
        fetches.append(
            pltpu.make_async_copy(ref, weights.at[:, pl.ds(256 * n, 256)], fetch_sem.at[n])
        )
        fetches[-1].start()
    fetch = pltpu.make_async_copy(out_w_ref, out_w, weight_sem)

    barrier = pltpu.get_barrier_semaphore()
    for ring in range(4):
        pl.semaphore_signal(
            barrier, inc=1, device_id={"sp": onward(ring // 2, ring % 2)}, device_id_type=MESH
        )
    for other in (twin, lax.rem(me + 1, 32), lax.rem(me + 31, 32)):
        pl.semaphore_signal(barrier, inc=1, device_id={"sp": other}, device_id_type=MESH)
    for hop in range(4):
        peer = lax.rem(group + hop, 4)
        pl.semaphore_signal(
            barrier, inc=1, device_id={"sp": partner, "tp": peer}, device_id_type=MESH
        )
        if hop > 0:
            pl.semaphore_signal(barrier, inc=1, device_id={"tp": peer}, device_id_type=MESH)

    for state in range(4):
        tops[state] = jnp.full((1, 512), NEG, jnp.float32)
        totals[state] = jnp.zeros((1, 512), jnp.float32)
        summed[state] = jnp.zeros((128, 512), jnp.float32)
    line = jnp.concatenate([qk_ref[0:1], qk_ref[1:2]], axis=1)
    column = jnp.broadcast_to(line, (128, 128)).T[:, 0:1]

    load.wait()
    pl.semaphore_wait(barrier, 14)
    for turn_ in range(2):
        near(0, turn_, group).start()
        near(1, 1 - turn_, group).start()
    for copy in fetches:
        copy.wait()
    fetch.start()

    def spread(state, side, block):
        upper = lax.broadcasted_iota(jnp.int32, (128, 128), 0) < 64
        zero = jnp.zeros((128, 128), jnp.bfloat16)
        places = pl.multiple_of(128 * side, 128)
        queries[state, :, pl.ds(places, 128)] = jnp.where(upper, block, zero)
        queries[state, :, pl.ds(places + 256, 128)] = jnp.where(upper, zero, block)

    def project(unit):
        block = block_of(unit)
        inputs = rows[block].astype(jnp.float32)
        power = jnp.mean(inputs * inputs, axis=-1, keepdims=True)
        normed = (inputs * lax.rsqrt(power + 1e-06) * norm_ref[...]).astype(jnp.bfloat16)
        places = pl.ds(pl.multiple_of(128 * block, 128), 128)
        cosine, sine = cosine_ref[:, places], sine_ref[:, places]

        def product(n):
            return jnp.dot(
                normed, weights[:, 256 * n : 256 * n + 256], preferred_element_type=jnp.float32
            ).astype(jnp.bfloat16).astype(jnp.float32)

        def prepared(flat, gains):
            parts = []
            for part in range(4):
                piece = flat[64 * part : 64 * part + 64]
                power = jnp.mean(piece * piece, axis=0, keepdims=True)
                piece = piece * lax.rsqrt(power + 1e-06)
                piece = piece * gains[64 * (part % 2) : 64 * (part % 2) + 64]
                first, second = piece[:32], piece[32:]
                parts.append(first * cosine - second * sine)
                parts.append(second * cosine + first * sine)
            return jnp.concatenate(parts, axis=0)

        keys = prepared(product(1).T, column).T.astype(jnp.bfloat16)
        values = product(2).T.astype(jnp.bfloat16)
        for head in range(2):
            part = slice(128 * head, 128 * head + 128)
            kv[head, me, unit, 0:128, :] = keys[:, part]
            kv[head, me, unit, 128:256, :] = values[part, :]
        turned = prepared(product(0).T, column * (64 ** (-0.5) * LOG2E)).astype(jnp.bfloat16)

        @pl.when(unit < 2)
        def _():
            for head in range(2):
                spread(head, unit, turned[128 * head : 128 * head + 128])

        @pl.when(unit >= 2)
        def _():
            for head in range(2):
                odd[unit - 2, head] = turned[128 * head : 128 * head + 128]

        gate = (product(3) * jax.nn.sigmoid(product(4))).astype(jnp.bfloat16)
        gated[places, :] = gate
        start = pl.multiple_of(128 * block + 32, 32)
        shifted[0, pl.ds(start, 128), :] = gate.astype(jnp.float32)
        for ring in range(4):
            ring_copy(ring, 1, unit).start()

        @pl.when((unit & 1) == 1)
        def _():
            for half in range(2):
                twin_copy(2 * half, 0, unit // 2, core).start()

    def advance(half, owner, chunk, masked):
        state = 2 * chunk + half
        spans = [(2 * owner + side, unit) for side in range(2) for unit in range(4)]
        keys = jnp.concatenate([kv[half, dev, unit, 0:128, :] for dev, unit in spans], axis=0)
        values = jnp.concatenate([kv[half, dev, unit, 128:256, :] for dev, unit in spans], axis=1)
        if masked:
            across = lax.broadcasted_iota(jnp.int32, (128, 256), 1)
            down = lax.broadcasted_iota(jnp.int32, (128, 256), 0)
            block = jnp.where(across < 128, block_of(2 * chunk), block_of(2 * chunk + 1))
            target = me + chunk * (31 - 2 * me)
            query_pos = 512 * target + 128 * block + (across & 127)
            allowed = jnp.concatenate(
                [down + 512 * dev + 128 * block_of(unit) <= query_pos for dev, unit in spans], axis=0
            )
        if masked:
            allowed = jnp.concatenate([allowed, allowed], axis=1)
        scores = jnp.dot(keys, queries[state], preferred_element_type=jnp.float32)
        scores = jnp.where(allowed, scores, 3.0 * NEG) if masked else scores
        before, sums_before = tops[state], totals[state]
        top = jnp.maximum(before, jnp.max(scores, axis=0, keepdims=True))
        shares = jnp.exp2(scores - top)
        factor = jnp.exp2(before - top)
        totals[state] = sums_before * factor + jnp.sum(shares, axis=0, keepdims=True)
        tops[state] = top
        summed[state] = summed[state] * factor + jnp.dot(
            values, shares.astype(jnp.bfloat16), preferred_element_type=jnp.float32
        )

    def target_of(chunk):
        return (me + chunk * (31 - 2 * me)) // 2

    def wanted(half, turned, step):
        owner = origin(half, turned // 2, step)
        return (owner <= target_of(1 - (turned & 1))).astype(jnp.int32)

    def compute(pending, done):
        early = pending[0] != 0
        bits = jnp.where(early, pending[0], pending[1])
        low = bits & (-bits)
        index = jnp.int32(0)
        for size, mask in ((1, 0xAAAAAA), (2, 0xCCCCCC), (4, 0xF0F0F0), (8, 0xFF00), (16, 0xFF0000)):
            index = index + size * ((low & mask) != 0).astype(jnp.int32)
        step = done - jnp.where(early, 5, 2) + index // 8
        turned, half = (index & 7) // 2, index & 1
        chunk = 1 - (turned & 1)
        direction = turned // 2
        owners = [origin(n, direction, step) for n in range(2)]
        owner = owners[0] + half * (owners[1] - owners[0])

        @pl.when(owner < target_of(chunk))
        def _():
            advance(half, owner, chunk, False)

        @pl.when(owner == target_of(chunk))
        def _():
            advance(half, owner, chunk, True)

        rest = bits & (bits - 1)
        return jnp.where(early, rest, pending[0]), jnp.where(early, pending[1], rest)

    def line_up():
        halo_copy.wait_recv()
        edge = halo[...].astype(jnp.float32)
        shifted[0, 0:32, :] = jnp.where(me == 0, jnp.zeros((32, 256), jnp.float32), edge)

    def line_up_by(shift):
        shifted[shift, 0:536, :] = shifted[0, shift : shift + 536, :]

    def conv_tile(tile, _):
        base = tile * 32
        total = jnp.zeros((32, 256), jnp.float32)
        for tap in range(31):
            offset = tap + 2
            start = pl.multiple_of(base + offset // 8 * 8, 8)
            total = total + taps_ref[tap : tap + 1, :] * shifted[offset % 8, pl.ds(start, 32), :]
        convolved[pl.ds(pl.multiple_of(base, 32), 32), :] = total
        return 0

    def add_up():
        lanes = lax.broadcasted_iota(jnp.int32, (512, 128), 1)
        conv_now = convolved[...]
        plain = jnp.sum(conv_now, axis=1, keepdims=True)
        square = jnp.sum(conv_now * conv_now, axis=1, keepdims=True)
        both = jnp.where(lanes == 0, plain, jnp.where(lanes == 1, square, 0.0))
        sums[0] = both.T[0:8]

    def normalize():
        for hop in range(1, 4):
            sums_copy(hop).wait_recv()
        total = sums[0] + sums[1] + sums[2] + sums[3]
        padded = jnp.concatenate([total, jnp.zeros((120, 512), jnp.float32)], axis=0).T
        middle = padded[:, 0:1] / 1024.0
        spread_now = padded[:, 1:2] / 1024.0 - middle * middle
        value = (convolved[...] - middle) * lax.rsqrt(spread_now + 1e-05)
        value = value * scale_ref[...] + shift_ref[...]
        conv_out[...] = (value * jax.nn.sigmoid(value)).astype(jnp.bfloat16)

    def mix(pieces, top_row, start, first=0, count=4):
        order = [lax.rem(group + hop, 4) for hop in range(4)]

        def columns(n, _):
            span = pl.ds(pl.multiple_of(512 * n, 512), 512)
            total = jnp.zeros((128, 512), jnp.float32) if start is None else start[:, span]
            for hop in range(4):
                rows = pl.ds(pl.multiple_of(top_row + 256 * order[hop], 256), 256)
                total = total + jnp.dot(
                    pieces[hop], out_w[rows, span], preferred_element_type=jnp.float32
                )
            if start is None:
                mixing[:, span] = total
            else:
                mixed_ref[:, span] = total.astype(jnp.bfloat16)
            return 0

        lax.fori_loop(first, first + count, columns, 0)

    def turn(t, pending):
        old, new = pending
        lap, unit = t // 4 + 1, lax.rem(t, 4)
        step = lap - jnp.where(unit == 0, 0, jnp.where(unit == 3, 1, 1))
        done = lap - 2

        @pl.when(t == 1)
        def _():
            near(0, 0, left).wait_recv()
            beyond(0, left).start()
            near(1, 1, right).wait_recv()
            beyond(1, right).start()

        @pl.when(t == 4)
        def _():
            near(1, 0, right).wait_recv()

        @pl.when(t == 5)
        def _():
            near(0, 1, left).wait_recv()

        @pl.when(t == 6)
        def _():
            beyond(0, far).wait_recv()
            beyond(1, far).wait_recv()

        @pl.when((t == 0) | (t == 4) | (t == 5) | (t == 6))
        def _():
            project(jnp.where(t == 0, 0, jnp.where(t == 6, 3, t - 3)))

        @pl.when(t == 6)
        def _():
            odd_copy.start()
            halo_copy.start()

        @pl.when((step >= 1) & (step < 8))
        def _():
            for ring in range(4):
                half, direction = ring // 2, ring % 2
                source = origin(half, direction, step) * 2 + core
                piece = kv.at[half, source, unit]
                pltpu.make_async_remote_copy(
                    src_ref=piece, dst_ref=piece,
                    send_sem=ring_send.at[ring, step - 1, unit],
                    recv_sem=ring_recv.at[ring, step - 1, unit],
                    device_id={"sp": ahead[ring]}, device_id_type=MESH,
                ).wait_recv()

                @pl.when(step < 7)
                def _():
                    pltpu.make_async_remote_copy(
                        src_ref=piece, dst_ref=piece,
                        send_sem=ring_send.at[ring, step, unit],
                        recv_sem=ring_recv.at[ring, step, unit],
                        device_id={"sp": ahead[ring]}, device_id_type=MESH,
                    ).start()

                @pl.when(step == 7)
                def _():
                    share = kv.at[half, source, unit, pl.ds(128 * direction, 128)]
                    pltpu.make_async_remote_copy(
                        src_ref=share, dst_ref=share,
                        send_sem=ring_send.at[ring, 7, unit], recv_sem=ring_recv.at[ring, 7, unit],
                        device_id={"sp": ahead[ring]}, device_id_type=MESH,
                    ).start()

            @pl.when((unit & 1) == 1)
            def _():
                for ring in (0, 2, 1, 3):
                    twin_copy(ring, step, unit // 2, core).start()

        @pl.when(step == 8)
        def _():
            for half in range(2):
                for direction in range(2):
                    ring_arrival(2 * half + direction, 8, unit, True).wait_recv()

                @pl.when((unit & 1) == 1)
                def _():
                    twin_copy(2 * half, 8, unit // 2, core).start()

        @pl.when(t == 8)
        def _():
            odd_copy.wait_recv()
            for side in range(2):
                for head in range(2):
                    spread(2 + head, side, odd_in[side, head])

            for half in range(2):
                for pair in range(2):
                    twin_copy(2 * half, 0, pair, 1 - core).wait_recv()

        for direction in range(2):

            @pl.when((done >= 1) & (unit == 2 * direction) & ((done < 8) | (direction == 0)))
            def _():
                for half in range(2):
                    for pair in range(2):
                        twin_copy(2 * half + direction, done, pair, 1 - core).wait_recv()

        old = jnp.where(unit == 0, old // 256 + (new & 255) * 65536, old)
        new = jnp.where(unit == 0, new // 256, new)
        for half in range(2):
            for turned in range(2):
                bit = 1 << (8 + 2 * turned + half)
                new = new + jnp.where(t == 8, bit * wanted(half, turned, 0), 0)
            valid = (done >= 1) & ((done < 8) | (unit < 2)) & (done <= 8)
            bit = jnp.where(unit == 0, 1, jnp.where(unit == 1, 4, jnp.where(unit == 2, 16, 64)))
            bit = bit * (65536 << half)
            step_now = jnp.clip(done, 0, 8)
            new = new + jnp.where(valid, bit * wanted(half, unit, step_now), 0)
        count = ((old + new) != 0).astype(jnp.int32) + (
            ((old & 255) != 0) & ((old & (old - 1)) != 0)
        ).astype(jnp.int32)
        old, new = lax.fori_loop(0, count, lambda n, words: compute(words, done), (old, new))

        @pl.when(t == 9)
        def _():
            line_up()

        for shift in range(1, 8):

            @pl.when(t == 9 + (shift + 1) // 2)
            def _():
                line_up_by(shift)

        @pl.when((t >= 14) & (t < 22))
        def _():
            lax.fori_loop(2 * t - 28, 2 * t - 26, conv_tile, 0)

        @pl.when(t == 22)
        def _():
            add_up()

        @pl.when(t == 23)
        def _():
            for hop in range(1, 4):
                sums_copy(hop).start()

        @pl.when(t == 28)
        def _():
            normalize()

        @pl.when(t == 29)
        def _():
            for hop in range(1, 4):
                conv_copy(hop).start()
            mine = pl.ds(pl.multiple_of(128 * group, 128), 128)
            conv_in[0] = conv_out[mine, :]

        @pl.when(t == 34)
        def _():
            fetch.wait()
            for hop in range(1, 4):
                conv_copy(hop).wait_recv()

        @pl.when((t >= 34) & (t < 38))
        def _():
            mix(conv_in, 1024, None, t - 34, 1)

        return old, new

    old, new = lax.fori_loop(0, 40, turn, (jnp.int32(0), jnp.int32(0)))

    def finish(chunk):
        for half in range(2):
            state = 2 * chunk + half
            share = summed[state] / totals[state]
            out = share[:, 0:256] - lam_ref[half] * share[:, 256:512]
            power = jnp.mean(out * out, axis=0, keepdims=True)
            out = (out * lax.rsqrt(power + 1e-06)).T * gain_ref[...]
            attended[chunk, :, 128 * half : 128 * half + 128] = out.astype(jnp.bfloat16)
            logs_in[chunk, half] = (tops[state] + jnp.log2(totals[state])) * (1.0 / LOG2E)

    def clear(mask):
        words = (old & mask, new & mask)
        count = jnp.int32(0)
        for n in range(24):
            for word in words:
                count = count + ((word & (1 << n)) != 0).astype(jnp.int32)
        lax.fori_loop(0, count, lambda n, left: compute(left, 8), words)

    clear(0x333333)
    finish(1)
    att_copy(3).start()
    att_copy(2).start()
    logs_copy.start()
    clear(0xCCCCCC)
    finish(0)
    att_copy(1).start()
    attended_in[0] = attended[0, 0:128, :]

    halo_copy.wait_send()
    odd_copy.wait_send()
    for hop in range(1, 4):
        sums_copy(hop).wait_send()
        conv_copy(hop).wait_send()
    for direction in range(2):
        for half in range(2):
            near(direction, half, group).wait_send()
        beyond(direction, left if direction == 0 else right).wait_send()

    def drain(step, _):
        for ring in range(4):
            for unit in range(4):
                ring_copy(ring, step, unit).wait_send()
            for pair in range(2):
                twin_copy(ring, step, pair, core).wait_send()
        return 0

    lax.fori_loop(1, 8, drain, 0)
    for half in range(2):
        for pair in range(2):
            twin_copy(2 * half, 0, pair, core).wait_send()
            twin_copy(2 * half, 8, pair, core).wait_send()
    for unit in range(4):
        for ring in range(4):
            ring_copy(ring, 8, unit, True).wait_send()
    logs_copy.wait()
    for unit in range(4):
        places = pl.ds(pl.multiple_of(128 * block_of(unit), 128), 128)
        for half in range(2):
            for m in range(2):
                start = 256 * m + 128 * (unit % 2)
                logs_ref[m, half : half + 1, places] = logs_in[
                    2 * (unit // 2), half, :, start : start + 128
                ]

    for unit in (1, 2, 3):
        att_copy(unit).wait_recv()
    mix(attended_in, 0, mixing)
    for unit in (1, 2, 3):
        att_copy(unit).wait_send()


def layer(*operands):
    vmem = pl.BlockSpec(memory_space=pltpu.VMEM)
    hbm = pl.BlockSpec(memory_space=pl.ANY)
    smem = pl.BlockSpec(memory_space=pltpu.SMEM)
    dma = pltpu.SemaphoreType.DMA
    bf16, f32 = jnp.bfloat16, jnp.float32
    return pl.pallas_call(
        layer_kernel,
        out_shape=(
            jax.ShapeDtypeStruct((128, 2048), bf16),
            jax.ShapeDtypeStruct((2, 2, 512), f32),
        ),
        in_specs=[hbm] * 6 + [vmem] * 4 + [smem] + [vmem] * 4 + [hbm],
        out_specs=(vmem, vmem),
        scratch_shapes=[
            pltpu.VMEM((4, 128, 2048), bf16),
            pltpu.VMEM((2048, 1280), bf16),
            pltpu.VMEM((2, 32, 4, 256, 128), bf16),
            pltpu.VMEM((2, 2, 128, 128), bf16),
            pltpu.VMEM((2, 2, 128, 128), bf16),
            pltpu.VMEM((4, 128, 512), bf16),
            pltpu.VMEM((4, 1, 512), f32),
            pltpu.VMEM((4, 1, 512), f32),
            pltpu.VMEM((4, 128, 512), f32),
            pltpu.VMEM((512, 256), bf16),
            pltpu.VMEM((32, 256), bf16),
            pltpu.VMEM((8, 544, 256), f32),
            pltpu.VMEM((512, 256), f32),
            pltpu.VMEM((4, 8, 512), f32),
            pltpu.VMEM((512, 256), bf16),
            pltpu.VMEM((4, 128, 256), bf16),
            pltpu.VMEM((2, 256, 256), bf16),
            pltpu.VMEM((4, 128, 256), bf16),
            pltpu.VMEM((3, 2, 1, 512), f32),
            pltpu.VMEM((2048, 2048), bf16),
            pltpu.VMEM((128, 2048), f32),
            dma, dma((5,)), dma((2, 2)), dma((2, 2)), dma((2,)), dma((2,)),
            dma((2,)), dma((4, 8, 4)), dma((4, 8, 4)), dma((4, 9, 2)), dma((4, 9, 2)),
            dma, dma((2,)), dma((4,)), dma((4,)), dma((4,)), dma((4,)), dma((4,)), dma((4,)), dma((2,)),
        ],
        compiler_params=pltpu.CompilerParams(
            collective_id=0, has_side_effects=True, vmem_limit_bytes=67043328,
        ),
    )(*operands)


def per_device(
    tokens,
    norm_gain,
    query_weight,
    key_weight,
    value_weight,
    glu_value_weight,
    glu_gate_weight,
    qk_gain,
    mix_lambda,
    head_gain,
    conv_kernel,
    channel_gain,
    channel_shift,
    output_weight,
):
    offset = lax.axis_index("sp") * 512
    positions = (offset + jnp.arange(512, dtype=jnp.int32)).astype(jnp.float32)
    inverse = 10000.0 ** (-jnp.arange(0, 32, dtype=jnp.float32) * 2.0 / 64)
    angles = inverse[:, None] * positions[None, :]
    return layer(
        tokens, query_weight, key_weight, value_weight, glu_value_weight, glu_gate_weight,
        norm_gain[None, :], qk_gain, jnp.cos(angles), jnp.sin(angles), mix_lambda, head_gain[None, :], conv_kernel,
        channel_gain[None, :], channel_shift[None, :], output_weight,
    )


def solution(mesh):
    placed = (
        P(("sp", "tp"), None),
        P(),
        P(None, "tp"),
        P(None, "tp"),
        P(None, "tp"),
        P(None, "tp"),
        P(None, "tp"),
        P(),
        P("tp"),
        P(),
        P(None, "tp"),
        P("tp"),
        P("tp"),
        P(),
    )
    return jax.shard_map(
        per_device,
        mesh=mesh,
        in_specs=placed,
        out_specs=(P(("sp", "tp"), None), P(None, "tp", "sp")),
        check_vma=False,
    )
```

```python
import jax
import jax.numpy as jnp
from jax import lax
from jax.experimental import pallas as pl
from jax.experimental.pallas import tpu as pltpu
from jax.sharding import PartitionSpec as P

MESH = pl.DeviceIdType.MESH
LOG2E = 1.4426950408889634
NEG = -1e30


def place(half, chip_z, chip_y):
    row = chip_z if half == 1 else chip_y
    return 4 * row + ((chip_y + chip_z) & 3)


def chip_at(half, position):
    row = position // 4
    other = (position + 12 - row) & 3
    return row * 4 + other if half == 1 else other * 4 + row


def layer_kernel(
    tok_ref, wq_ref, wk_ref, wv_ref, wa_ref, wg_ref, norm_ref, qk_ref, cosine_ref, sine_ref,
    lam_ref, gain_ref, taps_ref, scale_ref, shift_ref, out_w_ref,
    mixed_ref, logs_ref,
    rows, weights, kv, odd, odd_in, queries, tops, totals, summed,
    gated, halo, shifted, convolved, sums, conv_out, conv_in, attended, attended_in, logs_in,
    out_w, mixing,
    load_sem, fetch_sem, near_send, near_recv, far_send, far_recv,
    odd_sem, ring_send, ring_recv, twin_send, twin_recv,
    weight_sem, halo_sem, sums_send, sums_recv, conv_send, conv_recv, att_send, att_recv, logs_sem,
):
    me = lax.axis_index("sp")
    group = lax.axis_index("tp")
    core = lax.rem(me, 2)
    chip = me // 2
    chip_z, chip_y = chip // 4, lax.rem(chip, 4)
    twin = me + 1 - 2 * core
    partner = 31 - me
    right, left, far = (lax.rem(group + hop, 4) for hop in (1, 3, 2))

    def block_of(unit):
        return lax.rem(group + unit + unit // 2 - 2 * (unit // 3), 4)

    def origin(half, direction, step):
        here = place(half, chip_z, chip_y)
        there = (here + 16 - step + 2 * step * direction) & 15
        return chip_at(half, there)

    def onward(half, direction):
        here = place(half, chip_z, chip_y)
        there = (here + 17 - 2 * direction) & 15
        return chip_at(half, there) * 2 + core

    ahead = [onward(ring // 2, ring % 2) for ring in range(4)]

    def ring_piece(ring, source_step, step, unit, span):
        half, direction = ring // 2, ring % 2
        source = origin(half, direction, source_step) * 2 + core
        piece = kv.at[half, source, unit]
        if span is not None:
            piece = kv.at[half, source, unit, pl.ds(128 * direction, 128)]
        return pltpu.make_async_remote_copy(
            src_ref=piece, dst_ref=piece,
            send_sem=ring_send.at[ring, step - 1, unit],
            recv_sem=ring_recv.at[ring, step - 1, unit],
            device_id={"sp": ahead[ring]}, device_id_type=MESH,
        )

    def ring_copy(ring, step, unit, span=None):
        return ring_piece(ring, step - 1, step, unit, span)

    def ring_arrival(ring, step, unit, span=None):
        return ring_piece(ring, step, step, unit, span)

    def twin_copy(ring, step, pair, sender):
        half, direction = ring // 2, ring % 2
        source = origin(half, direction, step) * 2 + sender
        piece = kv.at[half, source, pl.ds(2 * pair, 2)]
        return pltpu.make_async_remote_copy(
            src_ref=piece, dst_ref=piece,
            send_sem=twin_send.at[ring, step, pair], recv_sem=twin_recv.at[ring, step, pair],
            device_id={"sp": twin}, device_id_type=MESH,
        )

    def hand(block, direction, half, send, recv):
        piece = rows.at[block, pl.ds(64 * half, 64)]
        return pltpu.make_async_remote_copy(
            src_ref=piece, dst_ref=piece, send_sem=send, recv_sem=recv,
            device_id={"tp": right if direction == 0 else left}, device_id_type=MESH,
        )

    def near(direction, half, block):
        return hand(
            block, direction, half, near_send.at[direction, half], near_recv.at[direction, half]
        )

    def beyond(direction, block):
        return hand(block, direction, direction, far_send.at[direction], far_recv.at[direction])

    odd_copy = pltpu.make_async_remote_copy(
        src_ref=odd, dst_ref=odd_in, send_sem=odd_sem.at[0], recv_sem=odd_sem.at[1],
        device_id={"sp": partner}, device_id_type=MESH,
    )
    halo_copy = pltpu.make_async_remote_copy(
        src_ref=gated.at[pl.ds(480, 32)], dst_ref=halo,
        send_sem=halo_sem.at[0], recv_sem=halo_sem.at[1],
        device_id={"sp": lax.rem(me + 1, 32)}, device_id_type=MESH,
    )
    logs_copy = pltpu.make_async_remote_copy(
        src_ref=logs_in.at[1], dst_ref=logs_in.at[2],
        send_sem=logs_sem.at[0], recv_sem=logs_sem.at[1],
        device_id={"sp": partner}, device_id_type=MESH,
    )

    def to_peers(source, target, send, recv, hop, count=None):
        peer = lax.rem(group + hop, 4)
        piece = source
        if count is not None:
            piece = source.at[pl.ds(pl.multiple_of(count * peer, 16), count)]
        return pltpu.make_async_remote_copy(
            src_ref=piece, dst_ref=target.at[4 - hop],
            send_sem=send.at[4 - hop], recv_sem=recv.at[4 - hop],
            device_id={"tp": peer}, device_id_type=MESH,
        )

    def sums_copy(hop):
        return to_peers(sums.at[0], sums, sums_send, sums_recv, hop)

    def conv_copy(hop):
        return to_peers(conv_out, conv_in, conv_send, conv_recv, hop, 128)

    def att_copy(unit):
        hop = (0, 1, 3, 2)[unit]
        return pltpu.make_async_remote_copy(
            src_ref=attended.at[unit // 2, pl.ds(128 * (unit % 2), 128)],
            dst_ref=attended_in.at[4 - hop],
            send_sem=att_send.at[4 - hop], recv_sem=att_recv.at[4 - hop],
            device_id={"sp": me if unit < 2 else partner, "tp": lax.rem(group + hop, 4)},
            device_id_type=MESH,
        )

    load = pltpu.make_async_copy(tok_ref, rows.at[group], load_sem)
    load.start()
    fetches = []
    for n, ref in enumerate((wq_ref, wk_ref, wv_ref, wa_ref, wg_ref)):
        fetches.append(
            pltpu.make_async_copy(ref, weights.at[:, pl.ds(256 * n, 256)], fetch_sem.at[n])
        )
        fetches[-1].start()
    fetch = pltpu.make_async_copy(out_w_ref, out_w, weight_sem)

    barrier = pltpu.get_barrier_semaphore()
    for ring in range(4):
        pl.semaphore_signal(
            barrier, inc=1, device_id={"sp": onward(ring // 2, ring % 2)}, device_id_type=MESH
        )
    for other in (twin, lax.rem(me + 1, 32), lax.rem(me + 31, 32)):
        pl.semaphore_signal(barrier, inc=1, device_id={"sp": other}, device_id_type=MESH)
    for hop in range(4):
        peer = lax.rem(group + hop, 4)
        pl.semaphore_signal(
            barrier, inc=1, device_id={"sp": partner, "tp": peer}, device_id_type=MESH
        )
        if hop > 0:
            pl.semaphore_signal(barrier, inc=1, device_id={"tp": peer}, device_id_type=MESH)

    for state in range(4):
        tops[state] = jnp.full((1, 512), NEG, jnp.float32)
        totals[state] = jnp.zeros((1, 512), jnp.float32)
        summed[state] = jnp.zeros((128, 512), jnp.float32)
    line = jnp.concatenate([qk_ref[0:1], qk_ref[1:2]], axis=1)
    column = jnp.broadcast_to(line, (128, 128)).T[:, 0:1]

    load.wait()
    pl.semaphore_wait(barrier, 14)
    for turn_ in range(2):
        near(0, turn_, group).start()
        near(1, 1 - turn_, group).start()
    for copy in fetches:
        copy.wait()
    fetch.start()

    def spread(state, side, block):
        upper = lax.broadcasted_iota(jnp.int32, (128, 128), 0) < 64
        zero = jnp.zeros((128, 128), jnp.bfloat16)
        places = pl.multiple_of(128 * side, 128)
        queries[state, :, pl.ds(places, 128)] = jnp.where(upper, block, zero)
        queries[state, :, pl.ds(places + 256, 128)] = jnp.where(upper, zero, block)

    def project(unit):
        block = block_of(unit)
        inputs = rows[block].astype(jnp.float32)
        power = jnp.mean(inputs * inputs, axis=-1, keepdims=True)
        normed = (inputs * lax.rsqrt(power + 1e-06) * norm_ref[...]).astype(jnp.bfloat16)
        places = pl.ds(pl.multiple_of(128 * block, 128), 128)
        cosine, sine = cosine_ref[:, places], sine_ref[:, places]

        def product(n):
            return jnp.dot(
                normed, weights[:, 256 * n : 256 * n + 256], preferred_element_type=jnp.float32
            ).astype(jnp.bfloat16).astype(jnp.float32)

        def prepared(flat, gains):
            parts = []
            for part in range(4):
                piece = flat[64 * part : 64 * part + 64]
                power = jnp.mean(piece * piece, axis=0, keepdims=True)
                piece = piece * lax.rsqrt(power + 1e-06)
                piece = piece * gains[64 * (part % 2) : 64 * (part % 2) + 64]
                first, second = piece[:32], piece[32:]
                parts.append(first * cosine - second * sine)
                parts.append(second * cosine + first * sine)
            return jnp.concatenate(parts, axis=0)

        keys = prepared(product(1).T, column).T.astype(jnp.bfloat16)
        values = product(2).T.astype(jnp.bfloat16)
        for head in range(2):
            part = slice(128 * head, 128 * head + 128)
            kv[head, me, unit, 0:128, :] = keys[:, part]
            kv[head, me, unit, 128:256, :] = values[part, :]
        turned = prepared(product(0).T, column * (64 ** (-0.5) * LOG2E)).astype(jnp.bfloat16)

        @pl.when(unit < 2)
        def _():
            for head in range(2):
                spread(head, unit, turned[128 * head : 128 * head + 128])

        @pl.when(unit >= 2)
        def _():
            for head in range(2):
                odd[unit - 2, head] = turned[128 * head : 128 * head + 128]

        for ring in range(4):
            ring_copy(ring, 1, unit).start()

        @pl.when((unit & 1) == 1)
        def _():
            for half in range(2):
                twin_copy(2 * half, 0, unit // 2, core).start()

        gate = (product(3) * jax.nn.sigmoid(product(4))).astype(jnp.bfloat16)
        gated[places, :] = gate
        start = pl.multiple_of(128 * block + 32, 32)
        shifted[0, pl.ds(start, 128), :] = gate.astype(jnp.float32)

    def advance(half, owner, chunk, masked):
        state = 2 * chunk + half
        spans = [(2 * owner + side, unit) for side in range(2) for unit in range(4)]
        keys = jnp.concatenate([kv[half, dev, unit, 0:128, :] for dev, unit in spans], axis=0)
        values = jnp.concatenate([kv[half, dev, unit, 128:256, :] for dev, unit in spans], axis=1)
        if masked:
            across = lax.broadcasted_iota(jnp.int32, (128, 256), 1)
            down = lax.broadcasted_iota(jnp.int32, (128, 256), 0)
            block = jnp.where(across < 128, block_of(2 * chunk), block_of(2 * chunk + 1))
            target = me + chunk * (31 - 2 * me)
            query_pos = 512 * target + 128 * block + (across & 127)
            allowed = jnp.concatenate(
                [down + 512 * dev + 128 * block_of(unit) <= query_pos for dev, unit in spans], axis=0
            )
        if masked:
            allowed = jnp.concatenate([allowed, allowed], axis=1)
        scores = jnp.dot(keys, queries[state], preferred_element_type=jnp.float32)
        scores = jnp.where(allowed, scores, 3.0 * NEG) if masked else scores
        before, sums_before = tops[state], totals[state]
        top = jnp.maximum(before, jnp.max(scores, axis=0, keepdims=True))
        shares = jnp.exp2(scores - top)
        factor = jnp.exp2(before - top)
        totals[state] = sums_before * factor + jnp.sum(shares, axis=0, keepdims=True)
        tops[state] = top
        summed[state] = summed[state] * factor + jnp.dot(
            values, shares.astype(jnp.bfloat16), preferred_element_type=jnp.float32
        )

    def target_of(chunk):
        return (me + chunk * (31 - 2 * me)) // 2

    def wanted(half, turned, step):
        owner = origin(half, turned // 2, step)
        return (owner <= target_of(1 - (turned & 1))).astype(jnp.int32)

    def compute(pending, done):
        early = pending[0] != 0
        bits = jnp.where(early, pending[0], pending[1])
        low = bits & (-bits)
        index = jnp.int32(0)
        for size, mask in ((1, 0xAAAAAA), (2, 0xCCCCCC), (4, 0xF0F0F0), (8, 0xFF00), (16, 0xFF0000)):
            index = index + size * ((low & mask) != 0).astype(jnp.int32)
        step = done - jnp.where(early, 5, 2) + index // 8
        turned, half = (index & 7) // 2, index & 1
        chunk = 1 - (turned & 1)
        direction = turned // 2
        owners = [origin(n, direction, step) for n in range(2)]
        owner = owners[0] + half * (owners[1] - owners[0])

        @pl.when(owner < target_of(chunk))
        def _():
            advance(half, owner, chunk, False)

        @pl.when(owner == target_of(chunk))
        def _():
            advance(half, owner, chunk, True)

        rest = bits & (bits - 1)
        return jnp.where(early, rest, pending[0]), jnp.where(early, pending[1], rest)

    def line_up():
        halo_copy.wait_recv()
        edge = halo[...].astype(jnp.float32)
        shifted[0, 0:32, :] = jnp.where(me == 0, jnp.zeros((32, 256), jnp.float32), edge)

    def line_up_by(shift):
        shifted[shift, 0:536, :] = shifted[0, shift : shift + 536, :]

    def conv_tile(tile, _):
        base = tile * 32
        total = jnp.zeros((32, 256), jnp.float32)
        for tap in range(31):
            offset = tap + 2
            start = pl.multiple_of(base + offset // 8 * 8, 8)
            total = total + taps_ref[tap : tap + 1, :] * shifted[offset % 8, pl.ds(start, 32), :]
        convolved[pl.ds(pl.multiple_of(base, 32), 32), :] = total
        return 0

    def add_up():
        lanes = lax.broadcasted_iota(jnp.int32, (512, 128), 1)
        conv_now = convolved[...]
        plain = jnp.sum(conv_now, axis=1, keepdims=True)
        square = jnp.sum(conv_now * conv_now, axis=1, keepdims=True)
        both = jnp.where(lanes == 0, plain, jnp.where(lanes == 1, square, 0.0))
        sums[0] = both.T[0:8]

    def normalize():
        for hop in range(1, 4):
            sums_copy(hop).wait_recv()
        total = sums[0] + sums[1] + sums[2] + sums[3]
        padded = jnp.concatenate([total, jnp.zeros((120, 512), jnp.float32)], axis=0).T
        middle = padded[:, 0:1] / 1024.0
        spread_now = padded[:, 1:2] / 1024.0 - middle * middle
        value = (convolved[...] - middle) * lax.rsqrt(spread_now + 1e-05)
        value = value * scale_ref[...] + shift_ref[...]
        conv_out[...] = (value * jax.nn.sigmoid(value)).astype(jnp.bfloat16)

    def mix(pieces, top_row, start, first=0, count=4):
        order = [lax.rem(group + hop, 4) for hop in range(4)]

        def columns(n, _):
            span = pl.ds(pl.multiple_of(512 * n, 512), 512)
            total = jnp.zeros((128, 512), jnp.float32) if start is None else start[:, span]
            for hop in range(4):
                rows = pl.ds(pl.multiple_of(top_row + 256 * order[hop], 256), 256)
                total = total + jnp.dot(
                    pieces[hop], out_w[rows, span], preferred_element_type=jnp.float32
                )
            if start is None:
                mixing[:, span] = total
            else:
                mixed_ref[:, span] = total.astype(jnp.bfloat16)
            return 0

        lax.fori_loop(first, first + count, columns, 0)

    def turn(t, pending):
        old, new = pending
        lap, unit = t // 4 + 1, lax.rem(t, 4)
        step = lap - jnp.where(unit == 0, 0, jnp.where(unit == 3, 1, 1))
        done = lap - 2

        @pl.when(t == 1)
        def _():
            near(0, 0, left).wait_recv()
            beyond(0, left).start()
            near(1, 1, right).wait_recv()
            beyond(1, right).start()

        @pl.when(t == 4)
        def _():
            near(1, 0, right).wait_recv()

        @pl.when(t == 5)
        def _():
            near(0, 1, left).wait_recv()

        @pl.when(t == 6)
        def _():
            beyond(0, far).wait_recv()
            beyond(1, far).wait_recv()

        @pl.when((t == 0) | (t == 4) | (t == 5) | (t == 6))
        def _():
            project(jnp.where(t == 0, 0, jnp.where(t == 6, 3, t - 3)))

        @pl.when(t == 6)
        def _():
            odd_copy.start()
            halo_copy.start()

        @pl.when((step >= 1) & (step < 8))
        def _():
            for ring in range(4):
                half, direction = ring // 2, ring % 2
                source = origin(half, direction, step) * 2 + core
                piece = kv.at[half, source, unit]
                pltpu.make_async_remote_copy(
                    src_ref=piece, dst_ref=piece,
                    send_sem=ring_send.at[ring, step - 1, unit],
                    recv_sem=ring_recv.at[ring, step - 1, unit],
                    device_id={"sp": ahead[ring]}, device_id_type=MESH,
                ).wait_recv()

                @pl.when(step < 7)
                def _():
                    pltpu.make_async_remote_copy(
                        src_ref=piece, dst_ref=piece,
                        send_sem=ring_send.at[ring, step, unit],
                        recv_sem=ring_recv.at[ring, step, unit],
                        device_id={"sp": ahead[ring]}, device_id_type=MESH,
                    ).start()

                @pl.when(step == 7)
                def _():
                    share = kv.at[half, source, unit, pl.ds(128 * direction, 128)]
                    pltpu.make_async_remote_copy(
                        src_ref=share, dst_ref=share,
                        send_sem=ring_send.at[ring, 7, unit], recv_sem=ring_recv.at[ring, 7, unit],
                        device_id={"sp": ahead[ring]}, device_id_type=MESH,
                    ).start()

            @pl.when((unit & 1) == 1)
            def _():
                for ring in (0, 2, 1, 3):
                    twin_copy(ring, step, unit // 2, core).start()

        @pl.when(step == 8)
        def _():
            for half in range(2):
                for direction in range(2):
                    ring_arrival(2 * half + direction, 8, unit, True).wait_recv()

                @pl.when((unit & 1) == 1)
                def _():
                    twin_copy(2 * half, 8, unit // 2, core).start()

        @pl.when(t == 8)
        def _():
            odd_copy.wait_recv()
            for side in range(2):
                for head in range(2):
                    spread(2 + head, side, odd_in[side, head])

            for half in range(2):
                for pair in range(2):
                    twin_copy(2 * half, 0, pair, 1 - core).wait_recv()

        for direction in range(2):

            @pl.when((done >= 1) & (unit == 2 * direction) & ((done < 8) | (direction == 0)))
            def _():
                for half in range(2):
                    for pair in range(2):
                        twin_copy(2 * half + direction, done, pair, 1 - core).wait_recv()

        old = jnp.where(unit == 0, old // 256 + (new & 255) * 65536, old)
        new = jnp.where(unit == 0, new // 256, new)
        for half in range(2):
            for turned in range(2):
                bit = 1 << (8 + 2 * turned + half)
                new = new + jnp.where(t == 8, bit * wanted(half, turned, 0), 0)
            valid = (done >= 1) & ((done < 8) | (unit < 2)) & (done <= 8)
            bit = jnp.where(unit == 0, 1, jnp.where(unit == 1, 4, jnp.where(unit == 2, 16, 64)))
            bit = bit * (65536 << half)
            step_now = jnp.clip(done, 0, 8)
            new = new + jnp.where(valid, bit * wanted(half, unit, step_now), 0)
        count = ((old + new) != 0).astype(jnp.int32) + (
            ((old & 255) != 0) & ((old & (old - 1)) != 0)
        ).astype(jnp.int32)
        old, new = lax.fori_loop(0, count, lambda n, words: compute(words, done), (old, new))

        @pl.when(t == 9)
        def _():
            line_up()

        for shift in range(1, 8):

            @pl.when(t == 9 + (shift + 1) // 2)
            def _():
                line_up_by(shift)

        @pl.when((t >= 14) & (t < 22))
        def _():
            lax.fori_loop(2 * t - 28, 2 * t - 26, conv_tile, 0)

        @pl.when(t == 22)
        def _():
            add_up()

        @pl.when(t == 23)
        def _():
            for hop in range(1, 4):
                sums_copy(hop).start()

        @pl.when(t == 28)
        def _():
            normalize()

        @pl.when(t == 29)
        def _():
            for hop in range(1, 4):
                conv_copy(hop).start()
            mine = pl.ds(pl.multiple_of(128 * group, 128), 128)
            conv_in[0] = conv_out[mine, :]

        @pl.when(t == 34)
        def _():
            fetch.wait()
            for hop in range(1, 4):
                conv_copy(hop).wait_recv()

        @pl.when((t >= 34) & (t < 38))
        def _():
            mix(conv_in, 1024, None, t - 34, 1)

        return old, new

    old, new = lax.fori_loop(0, 40, turn, (jnp.int32(0), jnp.int32(0)))

    def finish(chunk):
        for half in range(2):
            state = 2 * chunk + half
            share = summed[state] / totals[state]
            out = share[:, 0:256] - lam_ref[half] * share[:, 256:512]
            power = jnp.mean(out * out, axis=0, keepdims=True)
            out = (out * lax.rsqrt(power + 1e-06)).T * gain_ref[...]
            attended[chunk, :, 128 * half : 128 * half + 128] = out.astype(jnp.bfloat16)
            logs_in[chunk, half] = (tops[state] + jnp.log2(totals[state])) * (1.0 / LOG2E)

    def clear(mask):
        words = (old & mask, new & mask)
        count = jnp.int32(0)
        for n in range(24):
            for word in words:
                count = count + ((word & (1 << n)) != 0).astype(jnp.int32)
        lax.fori_loop(0, count, lambda n, left: compute(left, 8), words)

    clear(0x333333)
    finish(1)
    att_copy(3).start()
    att_copy(2).start()
    logs_copy.start()
    clear(0xCCCCCC)
    finish(0)
    att_copy(1).start()
    attended_in[0] = attended[0, 0:128, :]

    halo_copy.wait_send()
    odd_copy.wait_send()
    for hop in range(1, 4):
        sums_copy(hop).wait_send()
        conv_copy(hop).wait_send()
    for direction in range(2):
        for half in range(2):
            near(direction, half, group).wait_send()
        beyond(direction, left if direction == 0 else right).wait_send()

    def drain(step, _):
        for ring in range(4):
            for unit in range(4):
                ring_copy(ring, step, unit).wait_send()
            for pair in range(2):
                twin_copy(ring, step, pair, core).wait_send()
        return 0

    lax.fori_loop(1, 8, drain, 0)
    for half in range(2):
        for pair in range(2):
            twin_copy(2 * half, 0, pair, core).wait_send()
            twin_copy(2 * half, 8, pair, core).wait_send()
    for unit in range(4):
        for ring in range(4):
            ring_copy(ring, 8, unit, True).wait_send()
    logs_copy.wait()
    for unit in range(4):
        places = pl.ds(pl.multiple_of(128 * block_of(unit), 128), 128)
        for half in range(2):
            for m in range(2):
                start = 256 * m + 128 * (unit % 2)
                logs_ref[m, half : half + 1, places] = logs_in[
                    2 * (unit // 2), half, :, start : start + 128
                ]

    for unit in (1, 2, 3):
        att_copy(unit).wait_recv()
    mix(attended_in, 0, mixing)
    for unit in (1, 2, 3):
        att_copy(unit).wait_send()


def layer(*operands):
    vmem = pl.BlockSpec(memory_space=pltpu.VMEM)
    hbm = pl.BlockSpec(memory_space=pl.ANY)
    smem = pl.BlockSpec(memory_space=pltpu.SMEM)
    dma = pltpu.SemaphoreType.DMA
    bf16, f32 = jnp.bfloat16, jnp.float32
    return pl.pallas_call(
        layer_kernel,
        out_shape=(
            jax.ShapeDtypeStruct((128, 2048), bf16),
            jax.ShapeDtypeStruct((2, 2, 512), f32),
        ),
        in_specs=[hbm] * 6 + [vmem] * 4 + [smem] + [vmem] * 4 + [hbm],
        out_specs=(vmem, vmem),
        scratch_shapes=[
            pltpu.VMEM((4, 128, 2048), bf16),
            pltpu.VMEM((2048, 1280), bf16),
            pltpu.VMEM((2, 32, 4, 256, 128), bf16),
            pltpu.VMEM((2, 2, 128, 128), bf16),
            pltpu.VMEM((2, 2, 128, 128), bf16),
            pltpu.VMEM((4, 128, 512), bf16),
            pltpu.VMEM((4, 1, 512), f32),
            pltpu.VMEM((4, 1, 512), f32),
            pltpu.VMEM((4, 128, 512), f32),
            pltpu.VMEM((512, 256), bf16),
            pltpu.VMEM((32, 256), bf16),
            pltpu.VMEM((8, 544, 256), f32),
            pltpu.VMEM((512, 256), f32),
            pltpu.VMEM((4, 8, 512), f32),
            pltpu.VMEM((512, 256), bf16),
            pltpu.VMEM((4, 128, 256), bf16),
            pltpu.VMEM((2, 256, 256), bf16),
            pltpu.VMEM((4, 128, 256), bf16),
            pltpu.VMEM((3, 2, 1, 512), f32),
            pltpu.VMEM((2048, 2048), bf16),
            pltpu.VMEM((128, 2048), f32),
            dma, dma((5,)), dma((2, 2)), dma((2, 2)), dma((2,)), dma((2,)),
            dma((2,)), dma((4, 8, 4)), dma((4, 8, 4)), dma((4, 9, 2)), dma((4, 9, 2)),
            dma, dma((2,)), dma((4,)), dma((4,)), dma((4,)), dma((4,)), dma((4,)), dma((4,)), dma((2,)),
        ],
        compiler_params=pltpu.CompilerParams(
            collective_id=0, has_side_effects=True, vmem_limit_bytes=67043328,
        ),
    )(*operands)


def per_device(
    tokens,
    norm_gain,
    query_weight,
    key_weight,
    value_weight,
    glu_value_weight,
    glu_gate_weight,
    qk_gain,
    mix_lambda,
    head_gain,
    conv_kernel,
    channel_gain,
    channel_shift,
    output_weight,
):
    offset = lax.axis_index("sp") * 512
    positions = (offset + jnp.arange(512, dtype=jnp.int32)).astype(jnp.float32)
    inverse = 10000.0 ** (-jnp.arange(0, 32, dtype=jnp.float32) * 2.0 / 64)
    angles = inverse[:, None] * positions[None, :]
    return layer(
        tokens, query_weight, key_weight, value_weight, glu_value_weight, glu_gate_weight,
        norm_gain[None, :], qk_gain, jnp.cos(angles), jnp.sin(angles), mix_lambda, head_gain[None, :], conv_kernel,
        channel_gain[None, :], channel_shift[None, :], output_weight,
    )


def solution(mesh):
    placed = (
        P(("sp", "tp"), None),
        P(),
        P(None, "tp"),
        P(None, "tp"),
        P(None, "tp"),
        P(None, "tp"),
        P(None, "tp"),
        P(),
        P("tp"),
        P(),
        P(None, "tp"),
        P("tp"),
        P("tp"),
        P(),
    )
    return jax.shard_map(
        per_device,
        mesh=mesh,
        in_specs=placed,
        out_specs=(P(("sp", "tp"), None), P(None, "tp", "sp")),
        check_vma=False,
    )
```
